32 devices in a mesh: ep: 8 (over z, core), tp: 4 (over y, x).
Axes of the slice: x: 2, y: 2, z: 4, core: 2. Of those that a mesh axis runs over, the one named last changes fastest.
Arguments:
- query_rows: bfloat16 [4096, 2048], P('ep', 'tp'), may hold values from -6 to 6
- key_rows: bfloat16 [4096, 2048], P('ep', 'tp'), may hold values from -6 to 6
- value_rows: bfloat16 [4096, 4096], P('ep', 'tp'), may hold values from -6 to 6
- in_gate: float32 [16, 4096], P('tp', 'ep'), may hold values from -120 to 120
- forget_gate: float32 [16, 4096], P('tp', 'ep'), may hold values from -2 to 20
- out_gate: bfloat16 [4096, 4096], P('ep', 'tp'), may hold values from -6 to 6
- head_gain: float32 [4096], P('tp'), may hold values from 0.1 to 1.9
- mix_weight: bfloat16 [4096, 4096], P(None, 'tp'), may hold values from -0.09375 to 0.09375
- expert_input: bfloat16 [2048, 4096], P('ep', 'tp'), may hold values from -30 to 30
- routes: int32 [2048, 2], P('ep'), may hold values from 0 to 7, all different within a row; in each aligned block of 256 rows (0 to 255, 256 to 511, ...) at most 128 rows name the same one
- route_weight: float32 [2048, 2], P('ep'), may hold values from 0.25 to 1.25
- gate_weight: bfloat16 [8, 1024, 4096], P('ep', 'tp'), may hold values from -0.09375 to 0.09375
- up_weight: bfloat16 [8, 1024, 4096], P('ep', 'tp'), may hold values from -0.09375 to 0.09375
- down_weight: bfloat16 [8, 1024, 4096], P('ep', None, 'tp'), may hold values from -0.1875 to 0.1875
Outputs:
- mixer_out: bfloat16 [4096, 4096], P('ep', 'tp')
- expert_out: bfloat16 [2048, 4096], P('ep', 'tp')
The draws below stay inside these ranges and needn't reach their ends.
Inputs may be any that keep to these rules, and one draw needn't show every extreme that they name: `routes`: each row names 2 different experts. In the rows of one device no expert is named by more than 128 rows, and in the rows of some device an expert is named by exactly 128 rows.
All inputs are finite; a program needn't handle non-finite values.
Results may differ from the reference program's by a relative error of at most 0.0057.
Values may be sent and summed in bfloat16 or wider, within the bound.
A program may use at most 128 MiB of HBM per device.

```python
import math
import jax
import jax.numpy as jnp
import numpy as np
from jax import lax

D = 4096
HEADS = 16
QK = 128
FF = 1024
TOP = 2
BLOCK = 64
ROWS_A = 512
ROWS_B = 256
TOKENS_A = 4096
TOKENS_B = 2048
EXPERTS = 8
CAP = 128
N_EP = 8


def draw_in_gate(key, part):
    base = jnp.clip(jax.random.normal(jax.random.fold_in(key, 11), (HEADS, TOKENS_A), jnp.float32), -4.0, 4.0)
    return base


def draw_forget_gate(key, part):
    slow_share = 0.5
    slow_heads = jax.random.bernoulli(jax.random.fold_in(key, 21), slow_share, (HEADS, 1))
    level = jnp.where(slow_heads, math.log(TOKENS_A) + 0.5, 3.5)
    span_total = TOKENS_A // ROWS_A
    drift = jax.random.uniform(jax.random.fold_in(key, 22), (HEADS, span_total), jnp.float32, -1.0, 1.0)
    noise = 0.7 * jnp.clip(jax.random.normal(jax.random.fold_in(key, 23), (HEADS, TOKENS_A), jnp.float32), -4.0, 4.0)
    return level + jnp.repeat(drift, ROWS_A, axis=1) + noise


def draw_expert_input(key, part):
    row_scale = jnp.exp(jax.random.uniform(jax.random.fold_in(key, 31), (TOKENS_B, 1), jnp.float32, -0.7, 0.7))
    base = jnp.clip(jax.random.normal(jax.random.fold_in(key, 34), (TOKENS_B, D), jnp.float32), -4.0, 4.0)
    return (base * row_scale).astype(jnp.bfloat16)


def steps_of(rng, extent, split, low, high):
    loudness, own = 1.0, jax.random.fold_in(rng, 6)
    for axis_at, shards_of in split:
        steps = jnp.exp(jax.random.uniform(jax.random.fold_in(own, axis_at), (shards_of,), jnp.float32, low / len(split), high / len(split)))
        loudness = loudness * jnp.repeat(steps, extent[axis_at] // shards_of).reshape([-1 if axis == axis_at else 1 for axis in range(len(extent))])
    return loudness


def deal_out(key, own, number, rows, count, top, bound, slope):
    order = jax.random.permutation(key, count)
    packed, usual = load_shares(count, rows * top, bound, slope, True), load_shares(count, rows * top, bound, slope, False)
    places = jnp.arange(count)

    def named(tallies, offset_by):
        used = int((tallies > 0).sum())
        fixed = max(1, used // 4)
        shifted = fixed + (places - fixed + offset_by * (used - fixed)) % max(1, count - fixed)
        return jnp.zeros((count,), jnp.int32).at[order[jnp.where(places < fixed, places, shifted)]].set(jnp.asarray(tallies, jnp.int32))

    tallies = jnp.where(number % 4 == 0, named(packed, number // 4), named(usual, number - number // 4 - 1))
    mixed = jax.random.permutation(jax.random.fold_in(own, 3), count)
    donor, taker = mixed[0:count // 2 * 2:2], mixed[1:count // 2 * 2:2]
    room = jnp.minimum(tallies[donor] - 1, bound - tallies[taker]) // 2
    room = jnp.where((donor == order[0]) | (taker == order[0]) | (tallies[taker] == 0), 0, jnp.maximum(room, 0))
    shifted = jax.random.randint(jax.random.fold_in(own, 4), (count // 2,), 0, 1 << 20) % (room + 1)
    tallies = tallies.at[donor].add(-shifted).at[taker].add(shifted)
    labels = jnp.searchsorted(jnp.cumsum(tallies), jnp.arange(rows * top), side="right").astype(jnp.int32)
    listing = labels.reshape(top, rows).T
    listing = listing[jax.random.permutation(jax.random.fold_in(own, 1), rows)]
    offset_by = jax.random.randint(jax.random.fold_in(own, 2), (rows, 1), 0, top)
    return jnp.take_along_axis(listing, (jnp.arange(top)[None, :] + offset_by) % top, axis=1)


def load_shares(amount, total, bound, lean, full):
    weights = [(1 << 20) // math.isqrt(grade ** lean) + 1 for grade in range(1, amount + 1)]
    largest = bound if full else min(bound, max(-(-total // amount), total * weights[0] // sum(weights)))
    least = 1 if total - largest >= amount - 1 else 0
    given, rest = [largest] + [least] * (amount - 1), total - largest - least * (amount - 1)
    while rest > 0:
        free = [i for i in range(1, amount) if given[i] < largest] or [i for i in range(1, amount) if given[i] < bound]
        mass, remaining = sum([weights[i] for i in free]), rest
        for i in free:
            extra = min(bound - given[i], max(1, remaining * weights[i] // mass), rest)
            given[i] = given[i] + extra
            rest = rest - extra
    return np.array(given)


def centred(key, dims, scale, bound, cuts=(), kind=jnp.bfloat16):
    level = steps_of(key, dims, cuts, -0.22, 0.18) if cuts else 1.0
    entries = jax.random.normal(key, dims, jnp.float32) * scale * level
    return jnp.minimum(jnp.maximum(entries, -bound), bound).astype(kind)


def setup_inputs(seed: int = 0) -> dict:
    key_of = jax.random.split(jax.random.key(seed), 15)
    query_rows = centred(key_of[0], (TOKENS_A, HEADS * QK), 1.0, 6.0, ((0, 8), (1, 4)))
    key_rows = centred(key_of[1], (TOKENS_A, HEADS * QK), 1.0, 6.0, ((0, 8), (1, 4)))
    value_rows = centred(key_of[2], (TOKENS_A, D), 1.0, 6.0, ((0, 8), (1, 4)))
    in_gate = draw_in_gate(jax.random.fold_in(key_of[14], 71), 0)
    forget_gate = draw_forget_gate(jax.random.fold_in(key_of[14], 71), 0)
    out_gate = centred(key_of[5], (TOKENS_A, D), 1.0, 6.0, ((0, 8), (1, 4)))
    head_gain = jnp.clip(1.0 + 0.18 * jax.random.normal(key_of[6], (D,), jnp.float32), 0.1, 1.9)
    mix_weight = centred(key_of[7], (D, D), D ** -0.5, 0.09375, ((1, 4),))
    expert_input = draw_expert_input(jax.random.fold_in(key_of[14], 71), 0)
    routes_keys = jax.random.split(jax.random.fold_in(key_of[9], 1), TOKENS_B // ROWS_B)
    routes_turns = jax.random.permutation(jax.random.fold_in(key_of[9], 3), TOKENS_B // ROWS_B)
    routes = jax.vmap(lambda own, number: deal_out(jax.random.fold_in(key_of[9], 2), own, number, ROWS_B, EXPERTS, TOP, CAP, 1))(routes_keys, routes_turns).reshape((TOKENS_B, TOP))
    route_weight = jnp.clip(0.25 + 1.0 * jax.random.uniform(key_of[10], (TOKENS_B, TOP), jnp.float32) ** steps_of(key_of[10], (TOKENS_B, TOP), ((0, 8),), -0.2, 0.2), 0.25, 1.25)
    gate_weight = centred(key_of[11], (EXPERTS, FF, D), D ** -0.5, 0.09375, ((0, 8), (1, 4)))
    up_weight = centred(key_of[12], (EXPERTS, FF, D), D ** -0.5, 0.09375, ((0, 8), (1, 4)))
    down_weight = centred(key_of[13], (EXPERTS, FF, D), FF ** -0.5, 0.1875, ((0, 8), (2, 4)))
    return dict(query_rows=query_rows, key_rows=key_rows, value_rows=value_rows, in_gate=in_gate, forget_gate=forget_gate, out_gate=out_gate, head_gain=head_gain, mix_weight=mix_weight, expert_input=expert_input, routes=routes, route_weight=route_weight, gate_weight=gate_weight, up_weight=up_weight, down_weight=down_weight)


EPSILON = 1e-06
LOG_FLOOR = -1e+30
HIGHEST_PRECISION = lax.Precision.HIGHEST

def combine(first_part, second_part):
    decay_first, max_first, memory_first, normal_first = first_part
    decay_second, max_second, memory_second, normal_second = second_part
    running_max = jnp.maximum(decay_second + max_first, max_second)
    keep_first = jnp.exp(decay_second + max_first - running_max)
    keep_second = jnp.exp(max_second - running_max)
    memory = keep_first[..., None, None] * memory_first + keep_second[..., None, None] * memory_second
    normalizer = keep_first[..., None] * normal_first + keep_second[..., None] * normal_second
    return (decay_first + decay_second, running_max, memory, normalizer)

def identity_state(head_count, key_width, value_width):
    return (jnp.zeros((head_count,), jnp.float32), jnp.full((head_count,), LOG_FLOOR, jnp.float32), jnp.zeros((head_count, key_width, value_width), jnp.float32), jnp.zeros((head_count, key_width), jnp.float32))

def halfprod(form, left, right):
    return jnp.einsum(form, left.astype(jnp.float32), right.astype(jnp.float32), precision=HIGHEST_PRECISION)

def prepare(query_heads, key_heads, value_heads, in_gate, forget_gate):
    head_count, length, key_width = query_heads.shape
    block_count = length // BLOCK
    query_blocks = query_heads.reshape(head_count, block_count, BLOCK, key_width)
    key_blocks = key_heads.reshape(head_count, block_count, BLOCK, key_width)
    value_blocks = value_heads.reshape(head_count, block_count, BLOCK, value_heads.shape[-1])
    log_input = in_gate.reshape(head_count, block_count, BLOCK)
    cumulative = jnp.cumsum(jax.nn.log_sigmoid(forget_gate).reshape(head_count, block_count, BLOCK), axis=-1)
    block_decay = cumulative[..., -1]
    weight_log = block_decay[..., None] - cumulative + log_input
    block_max = lax.optimization_barrier(jnp.max(weight_log, axis=-1))
    weighted = key_blocks.astype(jnp.float32) * jnp.exp(weight_log - block_max[..., None])[..., None]
    normalizer = lax.optimization_barrier(jnp.sum(weighted, axis=2))
    memory = halfprod('hcsk,hcsv->hckv', weighted.astype(jnp.bfloat16), value_blocks)
    return ((query_blocks, key_blocks, value_blocks, log_input, cumulative), (block_decay, block_max, memory, normalizer))

def prefix(summary, initial):
    leading = jax.tree.map(lambda tensor: jnp.moveaxis(tensor, 1, 0), summary)

    def advance(running, current):
        return (combine(running, current), running)
    final_state, before = lax.scan(advance, initial, leading)
    return (final_state, jax.tree.map(lambda tensor: jnp.moveaxis(tensor, 0, 1), before))

def block_outputs(blocked, before):
    query_blocks, key_blocks, value_blocks, log_input, cumulative = blocked
    prior_max, prior_memory, prior_normal = (before[1], before[2], before[3])
    block_len = cumulative.shape[-1]
    scale = query_blocks.shape[-1] ** (-0.5)
    causal = jnp.tril(jnp.ones((block_len, block_len), dtype=bool))
    log_decay = jnp.where(causal, cumulative[..., :, None] - cumulative[..., None, :] + log_input[..., None, :], -jnp.inf)
    log_inter = cumulative + prior_max[..., None]
    top_value = jnp.maximum(log_inter, lax.optimization_barrier(jnp.max(log_decay, axis=-1)))
    scores = halfprod('hctk,hcsk->hcts', query_blocks, key_blocks) * scale * jnp.exp(log_decay - top_value[..., None])
    carried = jnp.exp(log_inter - top_value) * scale
    query_wide = query_blocks.astype(jnp.float32)
    numerator = carried[..., None] * jnp.einsum('hctk,hckv->hctv', query_wide, prior_memory, precision=HIGHEST_PRECISION) + halfprod('hcts,hcsv->hctv', scores.astype(jnp.bfloat16), value_blocks)
    denominator = carried * jnp.einsum('hctk,hck->hct', query_wide, prior_normal, precision=HIGHEST_PRECISION) + lax.optimization_barrier(jnp.sum(scores, axis=-1))
    return numerator / jnp.maximum(jnp.abs(denominator), jnp.exp(-top_value))[..., None]

def finish(head_values, out_gate, head_gain):
    head_count, block_count, block_len, value_width = head_values.shape
    per_head = jnp.transpose(head_values, (1, 2, 0, 3)).reshape(block_count * block_len, head_count, value_width)
    per_head = per_head * lax.rsqrt(lax.optimization_barrier(jnp.mean(per_head * per_head, axis=-1, keepdims=True)) + EPSILON)
    per_head = per_head.reshape(block_count * block_len, head_count * value_width) * head_gain
    per_head = per_head * jax.nn.sigmoid(out_gate.astype(jnp.float32))
    return per_head.astype(jnp.bfloat16)

def reference(query_rows, key_rows, value_rows, in_gate, forget_gate, out_gate, head_gain, mix_weight, expert_input, routes, route_weight, gate_weight, up_weight, down_weight):
    length = query_rows.shape[0]
    head_count = in_gate.shape[0]
    key_width = query_rows.shape[1] // head_count
    value_width = value_rows.shape[1] // head_count
    query_heads = query_rows.reshape(length, head_count, key_width).transpose(1, 0, 2)
    key_heads = key_rows.reshape(length, head_count, key_width).transpose(1, 0, 2)
    value_heads = value_rows.reshape(length, head_count, value_width).transpose(1, 0, 2)

    def one_head(current):
        query_one, key_one, value_one, input_one, forget_one = current
        blocked, summary = prepare(query_one[None], key_one[None], value_one[None], input_one[None], forget_one[None])
        final_state, before = prefix(summary, identity_state(1, key_width, value_width))
        return block_outputs(blocked, before)[0]
    head_values = lax.map(one_head, (query_heads, key_heads, value_heads, in_gate, forget_gate))
    mixed_heads = finish(head_values, out_gate, head_gain)
    mixer_out = jnp.dot(mixed_heads, mix_weight, preferred_element_type=jnp.float32).astype(jnp.bfloat16)
    squares = lax.optimization_barrier(jnp.sum(jnp.square(expert_input.astype(jnp.float32)), axis=-1))
    inverse_rms = lax.rsqrt(squares / D + EPSILON)
    slot_total = N_EP * CAP

    def one_expert(running, expert):
        matched = routes == expert
        picked = jnp.any(matched, axis=1)
        row_index = jnp.nonzero(picked, size=slot_total, fill_value=0)[0].astype(jnp.int32)
        count = jnp.sum(picked.astype(jnp.int32))
        is_valid = (jnp.arange(slot_total, dtype=jnp.int32) < count).astype(jnp.float32)
        weight = lax.optimization_barrier(jnp.sum(jnp.where(matched, route_weight, 0.0), axis=1))
        chosen = expert_input[row_index]
        row_scale = inverse_rms[row_index][:, None]
        gate_value = jnp.dot(chosen, gate_weight[expert].T, preferred_element_type=jnp.float32) * row_scale
        up_value = jnp.dot(chosen, up_weight[expert].T, preferred_element_type=jnp.float32) * row_scale
        hidden = (jax.nn.silu(gate_value) * up_value).astype(jnp.bfloat16)
        expert_rows = jnp.dot(hidden, down_weight[expert], preferred_element_type=jnp.float32).astype(jnp.bfloat16)
        term = expert_rows.astype(jnp.float32) * (weight[row_index] * is_valid)[:, None]
        return (running.at[row_index].add(term), None)
    total, _ = lax.scan(one_expert, jnp.zeros((TOKENS_B, D), jnp.float32), jnp.arange(EXPERTS, dtype=jnp.int32))
    return (mixer_out, total.astype(jnp.bfloat16))
```

```python
import functools

import jax
import jax.numpy as jnp
from jax import lax
from jax.experimental import pallas as pl
from jax.experimental.pallas import tpu as pltpu
from jax.sharding import PartitionSpec as P

EPSILON = 1e-06
LOG_FLOOR = -1e30
F32 = jnp.float32
BF16 = jnp.bfloat16
GROUPS = 8
PARTS = 4
PAD = 16


def flip(index, bits):
    place = 1
    while place <= bits:
        if bits & place:
            index = index + place * (1 - 2 * ((index // place) % 2))
        place *= 2
    return index


def flip_by(index, bits, size):
    place = 1
    while place < size:
        index = index + ((bits // place) % 2) * place * (1 - 2 * ((index // place) % 2))
        place *= 2
    return index


def dot(left, right, contract=((1,), (0,))):
    return lax.dot_general(left, right, (contract, ((), ())), preferred_element_type=F32)


def upright(row):
    size = row.shape[1]
    own = lax.broadcasted_iota(jnp.int32, (size, size), 0) == lax.broadcasted_iota(
        jnp.int32, (size, size), 1
    )
    return jnp.sum(jnp.where(own, row, jnp.zeros((), row.dtype)), axis=1, keepdims=True)


def scope(name):
    return jax.named_scope(name)


def kernel(
    ep,
    tp,
    head_count,
    model_width,
    x_ref,
    slot_row_ref,
    weight_ref,
    a_ref,
    cum_ref,
    gain_ref,
    q_hbm,
    k_hbm,
    v_hbm,
    og_hbm,
    wg_hbm,
    wu_hbm,
    wd_hbm,
    wm_hbm,
    mix_ref,
    exp_ref,
    q_ref,
    k_ref,
    v_ref,
    og_ref,
    wg_ref,
    wu_ref,
    wd_ref,
    wm_ref,
    slots,
    tok,
    hid,
    outb,
    ret,
    hm,
    local,
    st_in,
    st_out,
    load_sem,
    disp_send,
    disp_recv,
    tok_send,
    tok_recv,
    fwd_send,
    fwd_recv,
    hid_send,
    hid_recv,
    hidf_send,
    hidf_recv,
    ret_send,
    ret_recv,
    head_send,
    head_recv,
    hfwd_send,
    hfwd_recv,
    st_send,
    st_recv,
):
    me = lax.axis_index("ep")
    mine = lax.axis_index("tp")
    cap = slots.shape[0] // ep
    span = slots.shape[0] // GROUPS
    per = ep // GROUPS
    width = x_ref.shape[1]
    length = q_ref.shape[0]
    qk = q_ref.shape[1] // head_count
    vw = v_ref.shape[1] // head_count
    units = wg_ref.shape[0]
    square = tp == 4
    direct = (1, 2) if square else tuple(range(1, tp))

    loads = [
        pltpu.make_async_copy(source, target, load_sem.at[at])
        for at, (source, target) in enumerate(
            [
                (k_hbm, k_ref),
                (v_hbm, v_ref),
                (q_hbm, q_ref),
                (og_hbm, og_ref),
                (wg_hbm, wg_ref),
                (wu_hbm, wu_ref),
                (wd_hbm, wd_ref),
                (wm_hbm, wm_ref),
            ]
        )
    ]
    for load in loads:
        load.start()

    barrier = pltpu.get_barrier_semaphore()
    for i in range(1, ep):
        pl.semaphore_signal(barrier, inc=1, device_id={"ep": flip(me, i)})
    for j in range(1, tp):
        pl.semaphore_signal(barrier, inc=1, device_id={"tp": flip(mine, j)})

    tokens = x_ref.shape[0]

    def block(at, size):
        return pl.ds(pl.multiple_of(at * size, size), size)

    def pick(part, carry):
        size = slots.shape[0] // 4
        rows = part * size + lax.broadcasted_iota(jnp.int32, (size, tokens), 0)
        hit = (rows == slot_row_ref[0:1, :]) | (rows == slot_row_ref[1:2, :])
        chosen = dot(hit.astype(F32).astype(BF16), x_ref[...]).astype(BF16)
        slots[block(part, size), :] = chosen
        return carry

    with scope("pick"):
        lax.fori_loop(0, 4, pick, 0)
    tok[0, 0:cap, :] = slots[0:cap, :]
    with scope("barrier"):
        pl.semaphore_wait(barrier, ep - 1 + tp - 1)

    def dispatch(i):
        return pltpu.make_async_remote_copy(
            slots.at[block(i, cap)],
            tok.at[0, block(i, cap)],
            disp_send.at[i],
            disp_recv.at[i],
            device_id={"ep": flip_by(me, i, ep)},
        )

    def held(i):
        ahead = (me % 2 == 1) & (flip(me, i) > me)
        return ahead if i >= ep // 2 else ahead & (me < 2)

    def spread(group, j):
        return pltpu.make_async_remote_copy(
            tok.at[0, block(group, span)],
            tok.at[j, block(group, span)],
            tok_send.at[group, j],
            tok_recv.at[group, j],
            device_id={"tp": flip(mine, j)},
        )

    half = span // 2

    def onward(group, j):
        part = pl.ds(pl.multiple_of(group * span + (j - 1) * half, half), half)
        return pltpu.make_async_remote_copy(
            tok.at[j, part],
            tok.at[3, part],
            fwd_send.at[group, j],
            fwd_recv.at[group, j],
            device_id={"tp": flip(mine, 3 - j)},
        )

    def share(group, j):
        return pltpu.make_async_remote_copy(
            hid.at[0, block(group, span)],
            hid.at[j, block(group, span)],
            hid_send.at[group, j],
            hid_recv.at[group, j],
            device_id={"tp": flip(mine, j)},
        )

    def share_onward(group, j):
        part = pl.ds(pl.multiple_of(group * span + (j - 1) * half, half), half)
        return pltpu.make_async_remote_copy(
            hid.at[j, part],
            hid.at[3, part],
            hidf_send.at[group, j],
            hidf_recv.at[group, j],
            device_id={"tp": flip(mine, 3 - j)},
        )

    def give_back(i):
        return pltpu.make_async_remote_copy(
            outb.at[block(i, cap)],
            ret.at[block(i, cap)],
            ret_send.at[i],
            ret_recv.at[i],
            device_id={"ep": flip_by(me, i, ep)},
        )

    tile = length // PARTS

    def head_spread(part, j):
        rows = block(part, tile)
        return pltpu.make_async_remote_copy(
            hm.at[0, rows],
            hm.at[j, rows],
            head_send.at[part, j],
            head_recv.at[part, j],
            device_id={"tp": flip(mine, j)},
        )

    def head_onward(part, j):
        size = tile // 2
        rows = pl.ds(pl.multiple_of(part * tile + (j - 1) * size, size), size)
        return pltpu.make_async_remote_copy(
            hm.at[j, rows],
            hm.at[3, rows],
            hfwd_send.at[part, j],
            hfwd_recv.at[part, j],
            device_id={"tp": flip(mine, 3 - j)},
        )

    def chain(h):
        return pltpu.make_async_remote_copy(
            st_out.at[h],
            st_in.at[h],
            st_send.at[h],
            st_recv.at[h],
            device_id={"ep": me + 1},
        )

    def send_group(group):
        with scope("S"):
            for r in range(per):

                @pl.when(group * per + r > 0)
                def _():
                    dispatch(group * per + r).wait_recv()

        for j in direct:
            spread(group, j).start()

    def relay_group(group):
        if square:
            for j in direct:
                with scope("R"):
                    spread(group, j).wait_recv()
                onward(group, j).start()

    def collect_group(group):
        with scope("C"):
            for j in direct:
                (onward if square else spread)(group, j).wait_recv()

    def relay_share(group):
        if square:
            for j in direct:
                with scope("Q"):
                    share(group, j).wait_recv()
                share_onward(group, j).start()

    def expand(group):
        rows = block(group, span)
        gate = jnp.zeros((span, units), F32)
        up = jnp.zeros((span, units), F32)
        squares = jnp.zeros((span, 1), F32)
        for j in range(tp):
            piece = tok[j, rows, :]
            columns = pl.ds(pl.multiple_of(flip(mine, j) * width, width), width)
            gate += dot(piece, wg_ref[:, columns], ((1,), (1,)))
            up += dot(piece, wu_ref[:, columns], ((1,), (1,)))
            wide = piece.astype(F32)
            squares += jnp.sum(wide * wide, axis=1, keepdims=True)
        inverse = lax.rsqrt(squares / model_width + EPSILON)
        hid[0, rows, :] = (jax.nn.silu(gate * inverse) * (up * inverse)).astype(BF16)
        for j in direct:
            share(group, j).start()

    def contract(group):
        rows = block(group, span)
        with scope("K"):
            for j in direct:
                (share_onward if square else share)(group, j).wait_recv()
        total = jnp.zeros((span, width), F32)
        for j in range(tp):
            at = pl.ds(pl.multiple_of(flip(mine, j) * units, units), units)
            total += dot(hid[j, rows, :], wd_ref[at, :])
        outb[rows, :] = total.astype(BF16)
        for r in range(per):

            @pl.when(group * per + r > 0)
            def _():
                give_back(group * per + r).start()

    for i in range(1, ep):

        @pl.when(jnp.logical_not(held(i)))
        def _():
            dispatch(i).start()

    send_group(0)

    loads[0].wait()
    loads[1].wait()

    def summarise(h, carry):
        keys = k_ref[:, block(h, qk)]
        values = v_ref[:, block(h, vw)]
        log_in = a_ref[pl.ds(h, 1), :]
        top = jnp.max(log_in, axis=1, keepdims=True)
        weighted = keys.astype(F32) * jnp.exp(upright(log_in) - top)
        local[h, 0:qk, :] = dot(weighted.astype(BF16), values, ((0,), (0,)))
        normal = jnp.sum(weighted, axis=0, keepdims=True)
        local[h, qk : qk + 8, 0:qk] = jnp.broadcast_to(normal, (8, qk))
        decay = cum_ref[pl.ds(h, 1), :][:, length - 1 : length]
        local[h, qk + 8 : qk + 16, :] = jnp.broadcast_to(top + decay, (8, vw))
        return carry

    with scope("summarise"):
        lax.fori_loop(0, head_count, summarise, 0)

    @pl.when(me == 0)
    def _():
        st_in[:, 0 : qk + 8, :] = jnp.zeros((head_count, qk + 8, vw), F32)
        st_in[:, qk + 8 : qk + 16, :] = jnp.full((head_count, 8, vw), LOG_FLOOR, F32)

    def carry_on(h, carry):
        @pl.when(me > 0)
        def _():
            with scope("chainwait"):
                chain(h).wait_recv()

        decay = cum_ref[pl.ds(h, 1), :][:, length - 1 : length]
        carried_max = st_in[h, qk + 8 : qk + 9, :] + decay
        own_max = local[h, qk + 8 : qk + 9, :]
        new_max = jnp.maximum(carried_max, own_max)
        keep = jnp.exp(carried_max - new_max)
        add = jnp.exp(own_max - new_max)
        st_out[h, 0:qk, :] = keep * st_in[h, 0:qk, :] + add * local[h, 0:qk, :]
        st_out[h, qk : qk + 8, 0:qk] = (
            keep[:, 0:qk] * st_in[h, qk : qk + 8, 0:qk]
            + add[:, 0:qk] * local[h, qk : qk + 8, 0:qk]
        )
        st_out[h, qk : qk + 8, qk:vw] = jnp.zeros((8, vw - qk), F32)
        st_out[h, qk + 8 : qk + 16, :] = jnp.broadcast_to(new_max, (8, vw))

        @pl.when(me < ep - 1)
        def _():
            chain(h).start()

        return carry

    def heads(h, carry):
        columns = block(h, vw)
        queries = q_ref[:, block(h, qk)]
        keys = k_ref[:, block(h, qk)]
        scale = qk**-0.5
        causal = lax.broadcasted_iota(jnp.int32, (length, length), 1) <= lax.broadcasted_iota(
            jnp.int32, (length, length), 0
        )
        log_in = jnp.where(causal, a_ref[pl.ds(h, 1), :], -jnp.inf)
        prior_max = st_in[h, qk + 8 : qk + 9, 0:1]
        top = jnp.maximum(prior_max, jnp.max(log_in, axis=1, keepdims=True))
        scores = dot(queries, keys, ((1,), (1,))) * scale * jnp.exp(log_in - top)
        carried = jnp.exp(prior_max - top) * scale
        memory = st_in[h, 0:qk, :]
        high = memory.astype(BF16)
        low = (memory - high.astype(F32)).astype(BF16)
        numerator = carried * (dot(queries, high) + dot(queries, low)) + dot(
            scores.astype(BF16), v_ref[:, columns]
        )
        normal = st_in[h, qk : qk + 1, 0:qk]
        denominator = carried * jnp.sum(
            queries.astype(F32) * normal, axis=1, keepdims=True
        ) + jnp.sum(scores, axis=1, keepdims=True)
        floor = jnp.exp(-(upright(cum_ref[pl.ds(h, 1), :]) + top))
        value = numerator / jnp.maximum(jnp.abs(denominator), floor)
        value = value * lax.rsqrt(jnp.mean(value * value, axis=1, keepdims=True) + EPSILON)
        gate = jax.nn.sigmoid(og_ref[:, columns].astype(F32))
        hm[0, :, columns] = (value * gain_ref[:, columns] * gate).astype(BF16)
        return carry

    for at in range(2, 7):
        loads[at].wait()

    def when_between(step, low, high):
        return pl.when((step >= low) & (step <= high))

    quarter = me // (ep // 4)

    def step(k, carry):
        @pl.when(k < GROUPS - 1)
        def _():
            send_group(k + 1)

        @pl.when(k == quarter * (GROUPS // 4))
        def _():
            with scope("chain"):
                lax.fori_loop(0, head_count, carry_on, 0)
            for i in range(2, ep):

                @pl.when(held(i))
                def _():
                    dispatch(i).start()

            with scope("heads"):
                lax.fori_loop(0, head_count, heads, 0)

        @pl.when(k < GROUPS)
        def _():
            relay_group(k)

        @when_between(k, 1, GROUPS)
        def _():
            collect_group(k - 1)
            with scope("expand"):
                expand(k - 1)

        @when_between(k, GROUPS + 1, GROUPS + 2)
        def _():
            for j in direct:
                head_spread(k - GROUPS - 1, j).start()

        @when_between(k, 2, GROUPS + 1)
        def _():
            relay_share(k - 2)

        @pl.when(k >= 3)
        def _():
            contract(k - 3)

        return carry

    lax.fori_loop(0, GROUPS + 3, step, 0)
    for part in range(2, PARTS):
        for j in direct:
            head_spread(part, j).start()
    ret[0:cap, :] = outb[0:cap, :]

    def relay_heads(part):
        if square:
            for j in direct:
                with scope("HR"):
                    head_spread(part, j).wait_recv()
                head_onward(part, j).start()

    loads[7].wait()
    relay_heads(0)

    def combine():
        with scope("retwait"):
            for i in range(1, ep):
                give_back(i).wait_recv()
        places = lax.broadcasted_iota(jnp.int32, (slots.shape[0], tokens), 0)
        total = jnp.zeros((tokens, width), F32)
        for route in range(weight_ref.shape[0]):
            hit = places == slot_row_ref[route : route + 1, :]
            picked = dot(hit.astype(F32).astype(BF16), ret[...], ((0,), (0,)))
            total += picked * upright(weight_ref[route : route + 1, :])
        exp_ref[...] = total.astype(BF16)

    def mix(part, carry):
        @pl.when(part < PARTS - 1)
        def _():
            relay_heads(part + 1)

        @pl.when(part == PARTS - 1)
        def _():
            combine()

        with scope("M"):
            for j in direct:
                (head_onward if square else head_spread)(part, j).wait_recv()
        rows = block(part, tile)
        total = jnp.zeros((tile, width), F32)
        for j in range(tp):
            inputs = pl.ds(pl.multiple_of(flip(mine, j) * width, width), width)
            total += dot(hm[j, rows, :], wm_ref[inputs, :])
        mix_ref[rows, :] = total.astype(BF16)
        return carry

    lax.fori_loop(0, PARTS, mix, 0)

    for i in range(1, ep):
        dispatch(i).wait_send()
        give_back(i).wait_send()

    def finish_group(group, carry):
        for j in direct:
            spread(group, j).wait_send()
            share(group, j).wait_send()
            if square:
                onward(group, j).wait_send()
                share_onward(group, j).wait_send()
        return carry

    lax.fori_loop(0, GROUPS, finish_group, 0)

    def finish_part(part, carry):
        for j in direct:
            head_spread(part, j).wait_send()
            if square:
                head_onward(part, j).wait_send()
        return carry

    lax.fori_loop(0, PARTS, finish_part, 0)
    for h in range(head_count):

        @pl.when(me < ep - 1)
        def _():
            chain(h).wait_send()


def body(
    query_rows,
    key_rows,
    value_rows,
    in_gate,
    forget_gate,
    out_gate,
    head_gain,
    mix_weight,
    expert_input,
    routes,
    route_weight,
    gate_weight,
    up_weight,
    down_weight,
):
    ep, tp = lax.axis_size("ep"), lax.axis_size("tp")
    head_count, length = in_gate.shape
    token_count, fanout = routes.shape
    width = expert_input.shape[1]
    units = gate_weight.shape[1]
    capacity = 2 * token_count * fanout // ep
    slot_count = ep * capacity
    qk = query_rows.shape[1] // head_count
    vw = value_rows.shape[1] // head_count

    earlier = jnp.tril(jnp.ones((length, length), F32))
    cumulative = jnp.einsum(
        "hs,ts->ht", jax.nn.log_sigmoid(forget_gate), earlier, precision=lax.Precision.HIGHEST
    )
    shifted = in_gate - cumulative

    me = lax.axis_index("ep")
    turned = routes ^ me
    experts = jnp.arange(ep, dtype=jnp.int32)
    named = turned[:, :, None] == experts
    any_named = jnp.any(named, axis=1)
    before = jnp.dot(
        jnp.tril(jnp.ones((token_count, token_count), BF16), -1),
        any_named.astype(BF16),
        preferred_element_type=F32,
    ).astype(jnp.int32)
    places = experts * capacity + before
    slot_row = jnp.sum(jnp.where(named, places[:, None, :], 0), axis=2).T

    vmem = pl.BlockSpec(memory_space=pltpu.VMEM)
    anywhere = pl.BlockSpec(memory_space=pl.ANY)
    dma = pltpu.SemaphoreType.DMA
    gate_local, up_local, down_local = gate_weight[0], up_weight[0], down_weight[0]
    big = (query_rows, key_rows, value_rows, out_gate, gate_local, up_local, down_local, mix_weight)
    state = (head_count, qk + PAD, vw)
    return pl.pallas_call(
        functools.partial(kernel, ep, tp, head_count, mix_weight.shape[0]),
        out_shape=(
            jax.ShapeDtypeStruct((length, width), BF16),
            jax.ShapeDtypeStruct((token_count, width), BF16),
        ),
        in_specs=[vmem] * 6 + [anywhere] * 8,
        out_specs=(vmem, vmem),
        scratch_shapes=[pltpu.VMEM(array.shape, array.dtype) for array in big]
        + [
            pltpu.VMEM((slot_count, width), BF16),
            pltpu.VMEM((tp, slot_count, width), BF16),
            pltpu.VMEM((tp, slot_count, units), BF16),
            pltpu.VMEM((slot_count, width), BF16),
            pltpu.VMEM((slot_count, width), BF16),
            pltpu.VMEM((tp, length, width), BF16),
            pltpu.VMEM(state, F32),
            pltpu.VMEM(state, F32),
            pltpu.VMEM(state, F32),
            dma((8,)),
            dma((ep,)),
            dma((ep,)),
            dma((GROUPS, tp)),
            dma((GROUPS, tp)),
            dma((GROUPS, 4)),
            dma((GROUPS, 4)),
            dma((GROUPS, tp)),
            dma((GROUPS, tp)),
            dma((GROUPS, 4)),
            dma((GROUPS, 4)),
            dma((ep,)),
            dma((ep,)),
            dma((PARTS, tp)),
            dma((PARTS, tp)),
            dma((PARTS, 4)),
            dma((PARTS, 4)),
            dma((head_count,)),
            dma((head_count,)),
        ],
        compiler_params=pltpu.CompilerParams(
            collective_id=0, has_side_effects=True, vmem_limit_bytes=64000 * 1024
        ),
    )(
        expert_input,
        slot_row,
        route_weight.T,
        shifted,
        cumulative,
        head_gain[None, :],
        *big,
    )


def solution(mesh):
    in_specs = (
        P("ep", "tp"),
        P("ep", "tp"),
        P("ep", "tp"),
        P("tp", "ep"),
        P("tp", "ep"),
        P("ep", "tp"),
        P("tp"),
        P(None, "tp"),
        P("ep", "tp"),
        P("ep", None),
        P("ep", None),
        P("ep", "tp", None),
        P("ep", "tp", None),
        P("ep", None, "tp"),
    )
    out_specs = (P("ep", "tp"), P("ep", "tp"))
    return jax.shard_map(body, mesh=mesh, in_specs=in_specs, out_specs=out_specs, check_vma=False)
```

```python
import functools

import jax
import jax.numpy as jnp
from jax import lax
from jax.experimental import pallas as pl
from jax.experimental.pallas import tpu as pltpu
from jax.sharding import PartitionSpec as P

EPSILON = 1e-06
LOG_FLOOR = -1e30
F32 = jnp.float32
BF16 = jnp.bfloat16
PARTS = 4
PAD = 16


def flip(index, bits):
    place = 1
    while place <= bits:
        if bits & place:
            index = index + place * (1 - 2 * ((index // place) % 2))
        place *= 2
    return index


def flip_by(index, bits, size):
    place = 1
    while place < size:
        index = index + ((bits // place) % 2) * place * (1 - 2 * ((index // place) % 2))
        place *= 2
    return index


def dot(left, right, contract=((1,), (0,))):
    return lax.dot_general(left, right, (contract, ((), ())), preferred_element_type=F32)


def upright(row):
    size = row.shape[1]
    own = lax.broadcasted_iota(jnp.int32, (size, size), 0) == lax.broadcasted_iota(
        jnp.int32, (size, size), 1
    )
    return jnp.sum(jnp.where(own, row, jnp.zeros((), row.dtype)), axis=1, keepdims=True)


def scope(name):
    return jax.named_scope(name)


def kernel(
    ep,
    tp,
    head_count,
    model_width,
    x_ref,
    routes_ref,
    weight_ref,
    in_ref,
    forget_ref,
    gain_ref,
    q_hbm,
    k_hbm,
    v_hbm,
    og_hbm,
    wg_hbm,
    wu_hbm,
    wd_hbm,
    wm_hbm,
    mix_hbm,
    exp_hbm,
    q_ref,
    k_ref,
    v_ref,
    og_ref,
    wg_ref,
    wu_ref,
    wd_ref,
    wm_ref,
    mix_ref,
    exp_ref,
    a_ref,
    cum_ref,
    slot_row_ref,
    pos_ref,
    named_ref,
    rall,
    full,
    zraw,
    afull,
    tok,
    hid,
    outb,
    ret,
    hm,
    local,
    st_in,
    st_out,
    load_sem,
    out_sem,
    route_send,
    route_recv,
    own_send,
    own_recv,
    ownf_send,
    ownf_recv,
    part_send,
    part_recv,
    up_send,
    down_send,
    side_send,
    z_recv,
    a_send,
    a_side,
    a_recv,
    tok_send,
    tok_recv,
    fwd_send,
    fwd_recv,
    hid_send,
    hid_recv,
    hidf_send,
    hidf_recv,
    ret_send,
    ret_recv,
    head_send,
    head_recv,
    hfwd_send,
    hfwd_recv,
    st_send,
    st_recv,
):
    me = lax.axis_index("ep")
    mine = lax.axis_index("tp")
    span = outb.shape[0] // ep
    width = x_ref.shape[1]
    length = q_ref.shape[0]
    qk = q_ref.shape[1] // head_count
    vw = v_ref.shape[1] // head_count
    units = wg_ref.shape[0]
    square = tp == 4
    direct = (1, 2) if square else tuple(range(1, tp))

    loads = [
        pltpu.make_async_copy(source, target, load_sem.at[at])
        for at, (source, target) in enumerate(
            [
                (k_hbm, k_ref),
                (v_hbm, v_ref),
                (q_hbm, q_ref),
                (og_hbm, og_ref),
                (wg_hbm, wg_ref),
                (wu_hbm, wu_ref),
                (wd_hbm, wd_ref),
                (wm_hbm, wm_ref),
            ]
        )
    ]
    for load in loads:
        load.start()

    barrier = pltpu.get_barrier_semaphore()
    for i in range(1, ep):
        pl.semaphore_signal(barrier, inc=1, device_id={"ep": flip(me, i)})
    for j in range(1, tp):
        pl.semaphore_signal(barrier, inc=1, device_id={"tp": flip(mine, j)})

    tokens = x_ref.shape[0]

    def block(at, size):
        return pl.ds(pl.multiple_of(at * size, size), size)

    def route_copy(i):
        return pltpu.make_async_remote_copy(
            named_ref,
            rall.at[me],
            route_send.at[i],
            route_recv.at[i],
            device_id={"ep": flip(me, i)},
        )

    def route_arrival(i):
        source = flip(me, i)
        return pltpu.make_async_remote_copy(
            named_ref,
            rall.at[source],
            route_send.at[i],
            route_recv.at[i],
            device_id={"ep": source},
        )

    def own_spread(j, part):
        rows = pl.ds(part * (tokens // 2), tokens // 2)
        return pltpu.make_async_remote_copy(
            x_ref.at[rows],
            full.at[0, j, rows],
            own_send.at[j, part],
            own_recv.at[j, part],
            device_id={"tp": flip(mine, j)},
        )

    def own_onward(j):
        size = tokens // 2
        part = pl.ds((j - 1) * size, size)
        return pltpu.make_async_remote_copy(
            full.at[0, j, part],
            full.at[0, 3, part],
            ownf_send.at[j],
            ownf_recv.at[j],
            device_id={"tp": flip(mine, 3 - j)},
        )

    def to_partner(j):
        return pltpu.make_async_remote_copy(
            full.at[0, j] if j else x_ref,
            full.at[1, j],
            part_send.at[j],
            part_recv.at[j],
            device_id={"ep": flip(me, 1)},
        )

    def z_copy(source, target, sems, own=False):
        return pltpu.make_async_remote_copy(
            x_ref if own else zraw.at[source],
            zraw.at[source],
            sems.at[source],
            z_recv.at[source],
            device_id={"ep": target},
        )

    parity = me % 2
    last = ep - 1
    spare = flip(me - parity, 2)

    def wide_copy(j, target, sems, start_full):
        return pltpu.make_async_remote_copy(
            full.at[0, j] if start_full else afull.at[j],
            afull.at[j],
            sems.at[j],
            a_recv.at[j],
            device_id={"ep": target},
        )

    def index_of(place):
        middle = jnp.where(place == 2, 3 - parity, place + 1)
        return jnp.where(place < 2, place, jnp.where(place == last, 2 + parity, middle))

    routes = routes_ref[...].astype(F32)
    named_ref[0:2, :] = routes
    named_ref[2:8, :] = jnp.full((6, tokens), -1.0, F32)
    full[0, 0] = x_ref[...]
    with scope("barrier"):
        pl.semaphore_wait(barrier, ep - 1 + tp - 1)

    for step in range(2):
        for j in direct:
            own_spread(j, (j - 1 + step) % 2).start()
    for i in range(1, ep):
        route_copy(i).start()

    @pl.when(me < ep - 2)
    def _():
        z_copy(me, me + 2, up_send, own=True).start()

    @pl.when(me >= 2)
    def _():
        z_copy(me, me - 2, down_send, own=True).start()

    to_partner(0).start()
    rall[me] = named_ref[...]

    def spread(group, j):
        return pltpu.make_async_remote_copy(
            tok.at[0, block(group, span)],
            tok.at[j, block(group, span)],
            tok_send.at[group, j],
            tok_recv.at[group, j],
            device_id={"tp": flip(mine, j)},
        )

    half = span // 2

    def onward(group, j):
        part = pl.ds(pl.multiple_of(group * span + (j - 1) * half, half), half)
        return pltpu.make_async_remote_copy(
            tok.at[j, part],
            tok.at[3, part],
            fwd_send.at[group, j],
            fwd_recv.at[group, j],
            device_id={"tp": flip(mine, 3 - j)},
        )

    def share(group, j):
        return pltpu.make_async_remote_copy(
            hid.at[0, block(group, span)],
            hid.at[j, block(group, span)],
            hid_send.at[group, j],
            hid_recv.at[group, j],
            device_id={"tp": flip(mine, j)},
        )

    def share_onward(group, j):
        part = pl.ds(pl.multiple_of(group * span + (j - 1) * half, half), half)
        return pltpu.make_async_remote_copy(
            hid.at[j, part],
            hid.at[3, part],
            hidf_send.at[group, j],
            hidf_recv.at[group, j],
            device_id={"tp": flip(mine, 3 - j)},
        )

    def give_back(place, i):
        return pltpu.make_async_remote_copy(
            outb.at[block(place, span)],
            ret.at[block(i, span)],
            ret_send.at[i],
            ret_recv.at[i],
            device_id={"ep": flip_by(me, i, ep)},
        )

    tile = length // PARTS

    def head_spread(part, j):
        rows = block(part, tile)
        return pltpu.make_async_remote_copy(
            hm.at[0, rows],
            hm.at[j, rows],
            head_send.at[part, j],
            head_recv.at[part, j],
            device_id={"tp": flip(mine, j)},
        )

    def head_onward(part, j):
        size = tile // 2
        rows = pl.ds(pl.multiple_of(part * tile + (j - 1) * size, size), size)
        return pltpu.make_async_remote_copy(
            hm.at[j, rows],
            hm.at[3, rows],
            hfwd_send.at[part, j],
            hfwd_recv.at[part, j],
            device_id={"tp": flip(mine, 3 - j)},
        )

    def chain(h):
        return pltpu.make_async_remote_copy(
            st_out.at[h],
            st_in.at[h],
            st_send.at[h],
            st_recv.at[h],
            device_id={"ep": me + 1},
        )

    def pass_along(distance):
        below, above = me - 2 * distance, me + 2 * distance

        @pl.when(below >= 0)
        def _():
            with scope("F"):
                z_copy(below, me, up_send).wait_recv()

            @pl.when(me < ep - 2)
            def _():
                z_copy(below, me + 2, up_send).start()

            z_copy(below, flip(me, 1), side_send).start()

        @pl.when(above < ep)
        def _():
            with scope("F"):
                z_copy(above, me, down_send).wait_recv()

            @pl.when(me >= 2)
            def _():
                z_copy(above, me - 2, down_send).start()

            z_copy(above, flip(me, 1), side_send).start()

    def choose(source, rows):
        places = lax.broadcasted_iota(jnp.int32, (span, tokens), 0).astype(F32)
        hit = places == pos_ref[pl.ds(source, 1), :]
        return dot(hit.astype(F32).astype(BF16), rows).astype(BF16)

    def send_group(group):
        index = index_of(group)
        source = flip_by(me, index, ep)

        @pl.when(group == 2)
        def _():
            pass_along(1)

        @pl.when((group > 2) & (index % 2 == 0))
        def _():
            pass_along(index // 2)

        @pl.when(index % 2 == 1)
        def _():
            with scope("S"):
                z_copy(source, me, side_send).wait_recv()

        tok[0, block(group, span), :] = choose(source, zraw[source])
        for j in direct:
            spread(group, j).start()

    def relay_own():
        for j in direct:
            with scope("O"):
                own_spread(j, (j - 1) % 2).wait_recv()
            if square:
                own_onward(j).start()
        for j in direct:
            with scope("O"):
                own_spread(j, j % 2).wait_recv()
            to_partner(j).start()

    def take_own():
        if square:
            with scope("O"):
                for j in direct:
                    own_onward(j).wait_recv()
            to_partner(3).start()
        for j in range(tp):
            tok[j, 0:span, :] = choose(me, full[0, j])

    def take_wide():
        @pl.when(parity == 1)
        def _():
            with scope("A"):
                z_copy(spare, me, side_send).wait_recv()
                for j in range(1, tp):
                    wide_copy(j, me, a_side, False).wait_recv()

        rows = block(last, span)
        tok[0, rows, :] = choose(spare, zraw[spare])
        for j in range(1, tp):
            tok[j, rows, :] = choose(spare, afull[j])

    def take_partner():
        with scope("P"):
            for j in range(tp):
                to_partner(j).wait_recv()
        for j in range(tp):
            tok[j, span : 2 * span, :] = choose(flip(me, 1), full[1, j])

    def relay_group(group):
        if square:
            for j in direct:
                with scope("R"):
                    spread(group, j).wait_recv()
                onward(group, j).start()

    def collect_group(group):
        with scope("C"):
            for j in direct:
                (onward if square else spread)(group, j).wait_recv()

    def relay_share(group):
        if square:
            for j in direct:
                with scope("Q"):
                    share(group, j).wait_recv()
                share_onward(group, j).start()

    def expand(group):
        rows = block(group, span)
        gate = jnp.zeros((span, units), F32)
        up = jnp.zeros((span, units), F32)
        squares = jnp.zeros((span, 1), F32)
        for j in range(tp):
            piece = tok[j, rows, :]
            columns = pl.ds(pl.multiple_of(flip(mine, j) * width, width), width)
            gate += dot(piece, wg_ref[:, columns], ((1,), (1,)))
            up += dot(piece, wu_ref[:, columns], ((1,), (1,)))
            wide = piece.astype(F32)
            squares += jnp.sum(wide * wide, axis=1, keepdims=True)
        inverse = lax.rsqrt(squares / model_width + EPSILON)
        hid[0, rows, :] = (jax.nn.silu(gate * inverse) * (up * inverse)).astype(BF16)
        for j in direct:
            share(group, j).start()

    def contract(group):
        rows = block(group, span)
        with scope("K"):
            for j in direct:
                (share_onward if square else share)(group, j).wait_recv()
        total = jnp.zeros((span, width), F32)
        for j in range(tp):
            at = pl.ds(pl.multiple_of(flip(mine, j) * units, units), units)
            total += dot(hid[j, rows, :], wd_ref[at, :])
        outb[rows, :] = total.astype(BF16)

        @pl.when(group > 0)
        def _():
            give_back(group, index_of(group)).start()

    forget = forget_ref[...]
    decay_log = jnp.minimum(forget, 0.0) - jnp.log1p(jnp.exp(-jnp.abs(forget)))
    head_part = decay_log.astype(BF16)
    rest = decay_log - head_part.astype(F32)
    mid_part = rest.astype(BF16)
    low_part = (rest - mid_part.astype(F32)).astype(BF16)
    upper = lax.broadcasted_iota(jnp.int32, (length, length), 0) <= lax.broadcasted_iota(
        jnp.int32, (length, length), 1
    )
    upper = upper.astype(F32).astype(BF16)
    cumulative = dot(head_part, upper) + dot(mid_part, upper) + dot(low_part, upper)
    cum_ref[...] = cumulative
    a_ref[...] = in_ref[...] - cumulative

    strict = lax.broadcasted_iota(jnp.int32, (tokens, tokens), 0) < lax.broadcasted_iota(
        jnp.int32, (tokens, tokens), 1
    )
    strict = strict.astype(F32).astype(BF16)
    order = lax.broadcasted_iota(jnp.int32, (ep, tokens), 0)
    experts = (order ^ me).astype(F32)
    one = jnp.ones((ep, tokens), F32)
    none = jnp.zeros((ep, tokens), F32)
    first = jnp.where(experts == routes[0:1, :], one, none)
    second = jnp.where(experts == routes[1:2, :], one, none)
    places = (order * span).astype(F32) + dot((first + second).astype(BF16), strict)
    slot_row_ref[0:1, :] = jnp.sum(first * places, axis=0, keepdims=True)
    slot_row_ref[1:2, :] = jnp.sum(second * places, axis=0, keepdims=True)

    loads[0].wait()
    loads[1].wait()

    def summarise(h, carry):
        keys = k_ref[:, block(h, qk)]
        values = v_ref[:, block(h, vw)]
        log_in = a_ref[pl.ds(h, 1), :]
        top = jnp.max(log_in, axis=1, keepdims=True)
        weighted = keys.astype(F32) * jnp.exp(upright(log_in) - top)
        local[h, 0:qk, :] = dot(weighted.astype(BF16), values, ((0,), (0,)))
        normal = jnp.sum(weighted, axis=0, keepdims=True)
        local[h, qk : qk + 8, 0:qk] = jnp.broadcast_to(normal, (8, qk))
        decay = cum_ref[pl.ds(h, 1), :][:, length - 1 : length]
        local[h, qk + 8 : qk + 16, :] = jnp.broadcast_to(top + decay, (8, vw))
        return carry

    with scope("summarise"):
        lax.fori_loop(0, head_count, summarise, 0)

    @pl.when(me == 0)
    def _():
        st_in[:, 0 : qk + 8, :] = jnp.zeros((head_count, qk + 8, vw), F32)
        st_in[:, qk + 8 : qk + 16, :] = jnp.full((head_count, 8, vw), LOG_FLOOR, F32)

    def carry_on(h, carry):
        @pl.when(me > 0)
        def _():
            with scope("chainwait"):
                chain(h).wait_recv()

        decay = cum_ref[pl.ds(h, 1), :][:, length - 1 : length]
        carried_max = st_in[h, qk + 8 : qk + 9, :] + decay
        own_max = local[h, qk + 8 : qk + 9, :]
        new_max = jnp.maximum(carried_max, own_max)
        keep = jnp.exp(carried_max - new_max)
        add = jnp.exp(own_max - new_max)
        st_out[h, 0:qk, :] = keep * st_in[h, 0:qk, :] + add * local[h, 0:qk, :]
        st_out[h, qk : qk + 8, 0:qk] = (
            keep[:, 0:qk] * st_in[h, qk : qk + 8, 0:qk]
            + add[:, 0:qk] * local[h, qk : qk + 8, 0:qk]
        )
        st_out[h, qk : qk + 8, qk:vw] = jnp.zeros((8, vw - qk), F32)
        st_out[h, qk + 8 : qk + 16, :] = jnp.broadcast_to(new_max, (8, vw))

        @pl.when(me < ep - 1)
        def _():
            chain(h).start()

        return carry

    def heads(h, carry):
        columns = block(h, vw)
        queries = q_ref[:, block(h, qk)]
        keys = k_ref[:, block(h, qk)]
        scale = qk**-0.5
        causal = lax.broadcasted_iota(jnp.int32, (length, length), 1) <= lax.broadcasted_iota(
            jnp.int32, (length, length), 0
        )
        log_in = jnp.where(causal, a_ref[pl.ds(h, 1), :], -jnp.inf)
        prior_max = st_in[h, qk + 8 : qk + 9, 0:1]
        top = jnp.maximum(prior_max, jnp.max(log_in, axis=1, keepdims=True))
        scores = dot(queries, keys, ((1,), (1,))) * scale * jnp.exp(log_in - top)
        carried = jnp.exp(prior_max - top) * scale
        memory = st_in[h, 0:qk, :]
        high = memory.astype(BF16)
        low = (memory - high.astype(F32)).astype(BF16)
        numerator = carried * (dot(queries, high) + dot(queries, low)) + dot(
            scores.astype(BF16), v_ref[:, columns]
        )
        normal = st_in[h, qk : qk + 1, 0:qk]
        denominator = carried * jnp.sum(
            queries.astype(F32) * normal, axis=1, keepdims=True
        ) + jnp.sum(scores, axis=1, keepdims=True)
        floor = jnp.exp(-(upright(cum_ref[pl.ds(h, 1), :]) + top))
        value = numerator / jnp.maximum(jnp.abs(denominator), floor)
        value = value * lax.rsqrt(jnp.mean(value * value, axis=1, keepdims=True) + EPSILON)
        gate = jax.nn.sigmoid(og_ref[:, columns].astype(F32))
        hm[0, :, columns] = (value * gain_ref[:, columns] * gate).astype(BF16)
        return carry

    for at in range(2, 7):
        loads[at].wait()

    with scope("routes"):
        for i in range(1, ep):
            route_arrival(i).wait_recv()
    wanted = jnp.zeros((ep, tokens), F32) + me.astype(F32)
    named = (rall[:, 0, :] == wanted) | (rall[:, 1, :] == wanted)
    ahead = dot(jnp.where(named, one, none).astype(BF16), strict)
    pos_ref[...] = jnp.where(named, ahead, -one)

    def when_between(step, low, high):
        return pl.when((step >= low) & (step <= high))

    quarter = me // (ep // 4)

    def step(k, carry):
        @when_between(k, 1, ep - 3)
        def _():
            send_group(k + 1)

        @pl.when((k == 3) & (parity == 0))
        def _():
            for j in range(1, tp):
                wide_copy(j, flip(me, 2), a_send, True).start()

        @pl.when((k == last - 1) & (parity == 0))
        def _():
            for j in range(1, tp):
                with scope("A"):
                    wide_copy(j, me, a_send, False).wait_recv()
                wide_copy(j, flip(me, 1), a_side, False).start()

        @pl.when(k == quarter * (ep // 4))
        def _():
            with scope("chain"):
                lax.fori_loop(0, head_count, carry_on, 0)

        @pl.when(k == quarter * (ep // 4) + 1)
        def _():
            with scope("heads"):
                lax.fori_loop(0, head_count, heads, 0)

        @pl.when(k == 0)
        def _():
            relay_own()

        @when_between(k, 2, last - 1)
        def _():
            relay_group(k)

        @pl.when(k == 1)
        def _():
            take_own()

        @pl.when(k == 2)
        def _():
            take_partner()

        @when_between(k, 3, last)
        def _():
            collect_group(k - 1)

        @pl.when(k == ep)
        def _():
            take_wide()

        @when_between(k, 1, ep)
        def _():
            with scope("expand"):
                expand(k - 1)

        @when_between(k, ep + 1, ep + 2)
        def _():
            for j in direct:
                head_spread(k - ep - 1, j).start()

        @when_between(k, 2, ep + 1)
        def _():
            relay_share(k - 2)

        @pl.when(k >= 3)
        def _():
            contract(k - 3)

        return carry

    lax.fori_loop(0, ep + 3, step, 0)
    for part in range(2, PARTS):
        for j in direct:
            head_spread(part, j).start()
    ret[0:span, :] = outb[0:span, :]

    def relay_heads(part):
        if square:
            for j in direct:
                with scope("HR"):
                    head_spread(part, j).wait_recv()
                head_onward(part, j).start()

    loads[7].wait()
    relay_heads(0)

    def mix_out(part):
        rows = block(part, tile)
        return pltpu.make_async_copy(mix_ref.at[rows], mix_hbm.at[rows], out_sem.at[part])

    exp_out = pltpu.make_async_copy(exp_ref, exp_hbm, out_sem.at[PARTS])

    def settle():
        for i in range(1, ep):
            route_copy(i).wait_send()
        for j in direct:
            own_spread(j, 0).wait_send()
            own_spread(j, 1).wait_send()
            if square:
                own_onward(j).wait_send()
        for j in range(tp):
            to_partner(j).wait_send()

        @pl.when(parity == 0)
        def _():
            for j in range(1, tp):
                wide_copy(j, flip(me, 2), a_send, True).wait_send()
                wide_copy(j, flip(me, 1), a_side, False).wait_send()

        for distance in range(ep // 2):
            below, above = me - 2 * distance, me + 2 * distance
            own = distance == 0

            @pl.when((below >= 0) & (me < ep - 2))
            def _():
                z_copy(below, me + 2, up_send, own).wait_send()

            @pl.when((above < ep) & (me >= 2))
            def _():
                z_copy(above, me - 2, down_send, own).wait_send()

            if not own:

                @pl.when(below >= 0)
                def _():
                    z_copy(below, flip(me, 1), side_send).wait_send()

                @pl.when(above < ep)
                def _():
                    z_copy(above, flip(me, 1), side_send).wait_send()


        def finish_group(group, carry):
            for j in direct:
                share(group, j).wait_send()
                if square:
                    share_onward(group, j).wait_send()

            @pl.when((group >= 2) & (group < last))
            def _():
                for j in direct:
                    spread(group, j).wait_send()
                    if square:
                        onward(group, j).wait_send()

            return carry

        lax.fori_loop(0, ep, finish_group, 0)

        for h in range(head_count):

            @pl.when(me < ep - 1)
            def _():
                chain(h).wait_send()

    def combine():
        with scope("retwait"):
            for i in range(1, ep):
                give_back(i, i).wait_recv()
        places = lax.broadcasted_iota(jnp.int32, (ret.shape[0], tokens), 0).astype(F32)
        total = jnp.zeros((tokens, width), F32)
        for route in range(weight_ref.shape[0]):
            hit = places == slot_row_ref[route : route + 1, :]
            picked = dot(hit.astype(F32).astype(BF16), ret[...], ((0,), (0,)))
            total += picked * upright(weight_ref[route : route + 1, :])
        exp_ref[...] = total.astype(BF16)
        exp_out.start()

    def mix(part, carry):
        @pl.when(part < PARTS - 1)
        def _():
            relay_heads(part + 1)

        @pl.when(part == 0)
        def _():
            settle()

        @pl.when(part == PARTS - 1)
        def _():
            combine()

        with scope("M"):
            for j in direct:
                (head_onward if square else head_spread)(part, j).wait_recv()
        rows = block(part, tile)
        total = jnp.zeros((tile, width), F32)
        for j in range(tp):
            inputs = pl.ds(pl.multiple_of(flip(mine, j) * width, width), width)
            total += dot(hm[j, rows, :], wm_ref[inputs, :])
        mix_ref[rows, :] = total.astype(BF16)
        mix_out(part).start()
        return carry

    lax.fori_loop(0, PARTS, mix, 0)

    with scope("fin1"):
        for i in range(1, ep):
            give_back(i, i).wait_send()

    def finish_part(part, carry):
        mix_out(part).wait()
        for j in direct:
            head_spread(part, j).wait_send()
            if square:
                head_onward(part, j).wait_send()
        return carry

    with scope("fin2"):
        lax.fori_loop(0, PARTS, finish_part, 0)
        exp_out.wait()


def body(
    query_rows,
    key_rows,
    value_rows,
    in_gate,
    forget_gate,
    out_gate,
    head_gain,
    mix_weight,
    expert_input,
    routes,
    route_weight,
    gate_weight,
    up_weight,
    down_weight,
):
    ep, tp = lax.axis_size("ep"), lax.axis_size("tp")
    head_count, length = in_gate.shape
    token_count, fanout = routes.shape
    width = expert_input.shape[1]
    units = gate_weight.shape[1]
    capacity = 2 * token_count * fanout // ep
    slot_count = ep * capacity
    qk = query_rows.shape[1] // head_count
    vw = value_rows.shape[1] // head_count

    vmem = pl.BlockSpec(memory_space=pltpu.VMEM)
    anywhere = pl.BlockSpec(memory_space=pl.ANY)
    dma = pltpu.SemaphoreType.DMA
    gate_local, up_local, down_local = gate_weight[0], up_weight[0], down_weight[0]
    big = (query_rows, key_rows, value_rows, out_gate, gate_local, up_local, down_local, mix_weight)
    state = (head_count, qk + PAD, vw)
    return pl.pallas_call(
        functools.partial(kernel, ep, tp, head_count, mix_weight.shape[0]),
        out_shape=(
            jax.ShapeDtypeStruct((length, width), BF16),
            jax.ShapeDtypeStruct((token_count, width), BF16),
        ),
        in_specs=[vmem] * 6 + [anywhere] * 8,
        out_specs=(anywhere, anywhere),
        scratch_shapes=[pltpu.VMEM(array.shape, array.dtype) for array in big]
        + [
            pltpu.VMEM((length, width), BF16),
            pltpu.VMEM((token_count, width), BF16),
            pltpu.VMEM((head_count, length), F32),
            pltpu.VMEM((head_count, length), F32),
            pltpu.VMEM((fanout, token_count), F32),
            pltpu.VMEM((ep, token_count), F32),
            pltpu.VMEM((8, token_count), F32),
            pltpu.VMEM((ep, 8, token_count), F32),
            pltpu.VMEM((2, tp, token_count, width), BF16),
            pltpu.VMEM((ep, token_count, width), BF16),
            pltpu.VMEM((tp, token_count, width), BF16),
            pltpu.VMEM((tp, slot_count, width), BF16),
            pltpu.VMEM((tp, slot_count, units), BF16),
            pltpu.VMEM((slot_count, width), BF16),
            pltpu.VMEM((slot_count, width), BF16),
            pltpu.VMEM((tp, length, width), BF16),
            pltpu.VMEM(state, F32),
            pltpu.VMEM(state, F32),
            pltpu.VMEM(state, F32),
            dma((8,)),
            dma((PARTS + 1,)),
            dma((ep,)),
            dma((ep,)),
            dma((tp, 2)),
            dma((tp, 2)),
            dma((4,)),
            dma((4,)),
            dma((tp,)),
            dma((tp,)),
            dma((ep,)),
            dma((ep,)),
            dma((ep,)),
            dma((ep,)),
            dma((tp,)),
            dma((tp,)),
            dma((tp,)),
            dma((ep, tp)),
            dma((ep, tp)),
            dma((ep, 4)),
            dma((ep, 4)),
            dma((ep, tp)),
            dma((ep, tp)),
            dma((ep, 4)),
            dma((ep, 4)),
            dma((ep,)),
            dma((ep,)),
            dma((PARTS, tp)),
            dma((PARTS, tp)),
            dma((PARTS, 4)),
            dma((PARTS, 4)),
            dma((head_count,)),
            dma((head_count,)),
        ],
        compiler_params=pltpu.CompilerParams(
            collective_id=0, has_side_effects=True, vmem_limit_bytes=64000 * 1024
        ),
    )(
        expert_input,
        routes.T,
        route_weight.T,
        in_gate,
        forget_gate,
        head_gain[None, :],
        *big,
    )


def solution(mesh):
    in_specs = (
        P("ep", "tp"),
        P("ep", "tp"),
        P("ep", "tp"),
        P("tp", "ep"),
        P("tp", "ep"),
        P("ep", "tp"),
        P("tp"),
        P(None, "tp"),
        P("ep", "tp"),
        P("ep", None),
        P("ep", None),
        P("ep", "tp", None),
        P("ep", "tp", None),
        P("ep", None, "tp"),
    )
    out_specs = (P("ep", "tp"), P("ep", "tp"))
    return jax.shard_map(body, mesh=mesh, in_specs=in_specs, out_specs=out_specs, check_vma=False)
```

```python
import functools

import jax
import jax.numpy as jnp
from jax import lax
from jax.experimental import pallas as pl
from jax.experimental.pallas import tpu as pltpu
from jax.sharding import PartitionSpec as P

EPSILON = 1e-06
LOG_FLOOR = -1e30
F32 = jnp.float32
BF16 = jnp.bfloat16
PARTS = 4
PAD = 16


def flip(index, bits):
    place = 1
    while place <= bits:
        if bits & place:
            index = index + place * (1 - 2 * ((index // place) % 2))
        place *= 2
    return index


def flip_by(index, bits, size):
    place = 1
    while place < size:
        index = index + ((bits // place) % 2) * place * (1 - 2 * ((index // place) % 2))
        place *= 2
    return index


def dot(left, right, contract=((1,), (0,))):
    return lax.dot_general(left, right, (contract, ((), ())), preferred_element_type=F32)


def upright(row):
    size = row.shape[1]
    own = lax.broadcasted_iota(jnp.int32, (size, size), 0) == lax.broadcasted_iota(
        jnp.int32, (size, size), 1
    )
    return jnp.sum(jnp.where(own, row, jnp.zeros((), row.dtype)), axis=1, keepdims=True)


def scope(name):
    return jax.named_scope(name)


def kernel(
    ep,
    tp,
    head_count,
    model_width,
    x_hbm,
    routes_hbm,
    weight_hbm,
    in_hbm,
    forget_hbm,
    gain_hbm,
    q_hbm,
    k_hbm,
    v_hbm,
    og_hbm,
    wg_hbm,
    wu_hbm,
    wd_hbm,
    wm_hbm,
    mix_ref,
    exp_ref,
    x_ref,
    routes_ref,
    weight_ref,
    in_ref,
    forget_ref,
    gain_ref,
    q_ref,
    k_ref,
    v_ref,
    og_ref,
    wg_ref,
    wu_ref,
    wd_ref,
    wm_ref,
    a_ref,
    cum_ref,
    slot_row_ref,
    pos_ref,
    named_ref,
    rall,
    full,
    zraw,
    afull,
    tok,
    hid,
    outb,
    ret,
    hm,
    local,
    st_in,
    st_out,
    partial,
    load_sem,
    sent,
    route_recv,
    own_recv,
    ownf_recv,
    part_recv,
    up_send,
    down_send,
    side_send,
    z_recv,
    a_recv,
    tok_recv,
    tok_rest,
    fwd_recv,
    hid_recv,
    hidf_recv,
    ret_recv,
    head_recv,
    head_rest,
    hfwd_recv,
    st_recv,
):
    me = lax.axis_index("ep")
    mine = lax.axis_index("tp")
    span = outb.shape[0] // ep
    width = x_ref.shape[1]
    length = q_ref.shape[0]
    qk = q_ref.shape[1] // head_count
    vw = v_ref.shape[1] // head_count
    units = wg_ref.shape[0]
    square = tp == 4
    direct = (1, 2) if square else tuple(range(1, tp))

    loads = [
        pltpu.make_async_copy(source, target, load_sem.at[at])
        for at, (source, target) in enumerate(
            [
                (x_hbm, x_ref),
                (routes_hbm, routes_ref),
                (forget_hbm, forget_ref),
                (in_hbm, in_ref),
                (weight_hbm, weight_ref),
                (gain_hbm, gain_ref),
                (k_hbm, k_ref),
                (v_hbm, v_ref),
                (q_hbm, q_ref),
                (og_hbm, og_ref),
                (wg_hbm, wg_ref),
                (wu_hbm, wu_ref),
                (wd_hbm, wd_ref),
                (wm_hbm, wm_ref),
            ]
        )
    ]
    barrier = pltpu.get_barrier_semaphore()
    for i in range(1, ep):
        pl.semaphore_signal(barrier, inc=1, device_id={"ep": flip(me, i)})
    for j in range(1, tp):
        pl.semaphore_signal(barrier, inc=1, device_id={"tp": flip(mine, j)})

    for load in loads:
        load.start()

    tokens = x_ref.shape[0]

    def block(at, size):
        return pl.ds(pl.multiple_of(at * size, size), size)

    def settled(ref, sem):
        return pltpu.make_async_remote_copy(ref, ref, sem, sem, device_id={"tp": flip(mine, 1)})

    def route_copy(i):
        return pltpu.make_async_remote_copy(
            named_ref,
            rall.at[me],
            sent.at[0],
            route_recv.at[0],
            device_id={"ep": flip(me, i)},
        )

    def own_spread(j, part):
        rows = pl.ds(part * (tokens // 2), tokens // 2)
        return pltpu.make_async_remote_copy(
            x_ref.at[rows],
            full.at[0, j, rows],
            sent.at[1],
            own_recv.at[j - 1, part],
            device_id={"tp": flip(mine, j)},
        )

    def own_onward(j):
        size = tokens // 2
        part = pl.ds((j - 1) * size, size)
        return pltpu.make_async_remote_copy(
            full.at[0, j, part],
            full.at[0, 3, part],
            sent.at[2],
            ownf_recv.at[j - 1],
            device_id={"tp": flip(mine, 3 - j)},
        )

    def to_partner(j):
        return pltpu.make_async_remote_copy(
            full.at[0, j] if j else x_ref,
            full.at[1, j],
            sent.at[3],
            part_recv.at[j],
            device_id={"ep": flip(me, 1)},
        )

    def z_copy(source, target, sems, own=False):
        return pltpu.make_async_remote_copy(
            x_ref if own else zraw.at[source],
            zraw.at[source],
            sems.at[source],
            z_recv.at[source],
            device_id={"ep": target},
        )

    parity = me % 2
    last = ep - 1
    spare = flip(me - parity, 2)

    def wide_copy(j, target, start_full):
        return pltpu.make_async_remote_copy(
            full.at[0, j] if start_full else afull.at[j],
            afull.at[j],
            sent.at[4 if start_full else 5],
            a_recv.at[j],
            device_id={"ep": target},
        )

    def index_of(place):
        middle = jnp.where(place == 2, 3 - parity, place + 1)
        return jnp.where(place < 2, place, jnp.where(place == last, 2 + parity, middle))

    loads[0].wait()
    loads[1].wait()
    routes = routes_ref[...].astype(F32)
    named_ref[0:2, :] = routes
    named_ref[2:8, :] = jnp.full((6, tokens), -1.0, F32)
    full[0, 0] = x_ref[...]
    with scope("barrier"):
        pl.semaphore_wait(barrier, ep - 1 + tp - 1)

    for step in range(2):
        for j in direct:
            own_spread(j, (j - 1 + step) % 2).start()
    for i in range(1, ep):
        route_copy(i).start()

    @pl.when(me < ep - 2)
    def _():
        z_copy(me, me + 2, up_send, own=True).start()

    @pl.when(me >= 2)
    def _():
        z_copy(me, me - 2, down_send, own=True).start()

    to_partner(0).start()
    rall[me] = named_ref[...]

    half = span // 2

    def piece(start, at, size):
        return pl.ds(pl.multiple_of(start + at * size, size), size)

    def spread(group, j, turn):
        rows = piece(group * span, (j - 1 + turn) % 2, half)
        return pltpu.make_async_remote_copy(
            tok.at[0, rows],
            tok.at[j, rows],
            sent.at[6],
            tok_rest.at[group - 2] if turn else tok_recv.at[group - 2, j - 1],
            device_id={"tp": flip(mine, j)},
        )

    def onward(group, j):
        part = piece(group * span, j - 1, half)
        return pltpu.make_async_remote_copy(
            tok.at[j, part],
            tok.at[3, part],
            sent.at[7],
            fwd_recv.at[group - 2],
            device_id={"tp": flip(mine, 3 - j)},
        )

    def share(group, j):
        return pltpu.make_async_remote_copy(
            hid.at[0, block(group, span)],
            hid.at[j, block(group, span)],
            sent.at[8],
            hid_recv.at[group, j - 1],
            device_id={"tp": flip(mine, j)},
        )

    def share_onward(group, j):
        part = piece(group * span, j - 1, half)
        return pltpu.make_async_remote_copy(
            hid.at[j, part],
            hid.at[3, part],
            sent.at[9],
            hidf_recv.at[group],
            device_id={"tp": flip(mine, 3 - j)},
        )

    def give_back(place, i):
        return pltpu.make_async_remote_copy(
            outb.at[block(place, span)],
            ret.at[block(i, span)],
            sent.at[10],
            ret_recv.at[0],
            device_id={"ep": flip_by(me, i, ep)},
        )

    tile = length // PARTS
    tile_half = tile // 2

    def head_spread(part, j, turn):
        rows = piece(part * tile, (j - 1 + turn) % 2, tile_half)
        return pltpu.make_async_remote_copy(
            hm.at[0, rows],
            hm.at[j, rows],
            sent.at[11],
            head_rest.at[part] if turn else head_recv.at[part, j - 1],
            device_id={"tp": flip(mine, j)},
        )

    def head_onward(part, j):
        rows = piece(part * tile, j - 1, tile_half)
        return pltpu.make_async_remote_copy(
            hm.at[j, rows],
            hm.at[3, rows],
            sent.at[12],
            hfwd_recv.at[part],
            device_id={"tp": flip(mine, 3 - j)},
        )

    def chain(h):
        return pltpu.make_async_remote_copy(
            st_out.at[h],
            st_in.at[h],
            sent.at[13],
            st_recv.at[h],
            device_id={"ep": me + 1},
        )

    many = pl.ds(0, len(direct))

    def pass_along(distance):
        below, above = me - 2 * distance, me + 2 * distance

        @pl.when(below >= 0)
        def _():
            with scope("F"):
                z_copy(below, me, up_send).wait_recv()

            @pl.when(me < ep - 2)
            def _():
                z_copy(below, me + 2, up_send).start()

            z_copy(below, flip(me, 1), side_send).start()

        @pl.when(above < ep)
        def _():
            with scope("F"):
                z_copy(above, me, down_send).wait_recv()

            @pl.when(me >= 2)
            def _():
                z_copy(above, me - 2, down_send).start()

            z_copy(above, flip(me, 1), side_send).start()

    def choose(source, rows):
        places = lax.broadcasted_iota(jnp.int32, (span, tokens), 0).astype(F32)
        hit = places == pos_ref[pl.ds(source, 1), :]
        return dot(hit.astype(F32).astype(BF16), rows).astype(BF16)

    def send_group(group):
        index = index_of(group)
        source = flip_by(me, index, ep)

        @pl.when(group == 2)
        def _():
            pass_along(1)

        @pl.when((group > 2) & (index % 2 == 0))
        def _():
            pass_along(index // 2)

        @pl.when(index % 2 == 1)
        def _():
            with scope("S"):
                z_copy(source, me, side_send).wait_recv()

        tok[0, block(group, span), :] = choose(source, zraw[source])
        for j in direct:
            spread(group, j, 0).start()

    def relay_own():
        for j in direct:
            with scope("O"):
                own_spread(j, (j - 1) % 2).wait_recv()
            if square:
                own_onward(j).start()
        for j in direct:
            with scope("O"):
                own_spread(j, j % 2).wait_recv()
            to_partner(j).start()

    def take_own():
        if square:
            with scope("O"):
                for j in direct:
                    own_onward(j).wait_recv()
            to_partner(3).start()
        for j in range(tp):
            tok[j, 0:span, :] = choose(me, full[0, j])

    def take_wide():
        @pl.when(parity == 1)
        def _():
            with scope("A"):
                z_copy(spare, me, side_send).wait_recv()
                for j in range(1, tp):
                    wide_copy(j, me, False).wait_recv()

        rows = block(last, span)
        tok[0, rows, :] = choose(spare, zraw[spare])
        for j in range(1, tp):
            tok[j, rows, :] = choose(spare, afull[j])

    def take_partner():
        with scope("P"):
            for j in range(tp):
                to_partner(j).wait_recv()
        for j in range(tp):
            tok[j, span : 2 * span, :] = choose(flip(me, 1), full[1, j])

    def relay_group(group):
        if square:
            for j in direct:
                with scope("R"):
                    spread(group, j, 0).wait_recv()
                onward(group, j).start()

    def collect_group(group):
        with scope("C"):
            if square:
                settled(tok.at[3, block(group, span)], fwd_recv.at[group - 2]).wait_recv()
            else:
                for j in direct:
                    spread(group, j, 0).wait_recv()
            settled(tok.at[many, piece(0, 0, half)], tok_rest.at[group - 2]).wait_recv()

    def relay_share(group):
        if square:
            for j in direct:
                with scope("Q"):
                    share(group, j).wait_recv()
                share_onward(group, j).start()

    def expand(group):
        rows = block(group, span)
        gate = jnp.zeros((span, units), F32)
        up = jnp.zeros((span, units), F32)
        squares = jnp.zeros((span, 1), F32)
        for j in range(tp):
            piece = tok[j, rows, :]
            columns = pl.ds(pl.multiple_of(flip(mine, j) * width, width), width)
            gate += dot(piece, wg_ref[:, columns], ((1,), (1,)))
            up += dot(piece, wu_ref[:, columns], ((1,), (1,)))
            wide = piece.astype(F32)
            squares += jnp.sum(wide * wide, axis=1, keepdims=True)
        inverse = lax.rsqrt(squares / model_width + EPSILON)
        hid[0, rows, :] = (jax.nn.silu(gate * inverse) * (up * inverse)).astype(BF16)
        for j in direct:
            share(group, j).start()

    def contract(group):
        rows = block(group, span)
        with scope("K"):
            if square:
                settled(hid.at[3, block(group, span)], hidf_recv.at[group]).wait_recv()
            else:
                for j in direct:
                    share(group, j).wait_recv()
        total = jnp.zeros((span, width), F32)
        for j in range(tp):
            at = pl.ds(pl.multiple_of(flip(mine, j) * units, units), units)
            total += dot(hid[j, rows, :], wd_ref[at, :])
        outb[rows, :] = total.astype(BF16)

        @pl.when(group > 0)
        def _():
            give_back(group, index_of(group)).start()

    for at in range(2, 6):
        loads[at].wait()
    forget = forget_ref[...]
    decay_log = jnp.minimum(forget, 0.0) - jnp.log1p(jnp.exp(-jnp.abs(forget)))
    head_part = decay_log.astype(BF16)
    rest = decay_log - head_part.astype(F32)
    mid_part = rest.astype(BF16)
    low_part = (rest - mid_part.astype(F32)).astype(BF16)
    upper = lax.broadcasted_iota(jnp.int32, (length, length), 0) <= lax.broadcasted_iota(
        jnp.int32, (length, length), 1
    )
    upper = upper.astype(F32).astype(BF16)
    cumulative = dot(head_part, upper) + dot(mid_part, upper) + dot(low_part, upper)
    cum_ref[...] = cumulative
    a_ref[...] = in_ref[...] - cumulative

    strict = lax.broadcasted_iota(jnp.int32, (tokens, tokens), 0) < lax.broadcasted_iota(
        jnp.int32, (tokens, tokens), 1
    )
    strict = strict.astype(F32).astype(BF16)
    order = lax.broadcasted_iota(jnp.int32, (ep, tokens), 0)
    experts = (order ^ me).astype(F32)
    one = jnp.ones((ep, tokens), F32)
    none = jnp.zeros((ep, tokens), F32)
    first = jnp.where(experts == routes[0:1, :], one, none)
    second = jnp.where(experts == routes[1:2, :], one, none)
    places = (order * span).astype(F32) + dot((first + second).astype(BF16), strict)
    slot_row_ref[0:1, :] = jnp.sum(first * places, axis=0, keepdims=True)
    slot_row_ref[1:2, :] = jnp.sum(second * places, axis=0, keepdims=True)

    loads[6].wait()
    loads[7].wait()

    def summarise(h, carry):
        keys = k_ref[:, block(h, qk)]
        values = v_ref[:, block(h, vw)]
        log_in = a_ref[pl.ds(h, 1), :]
        top = jnp.max(log_in, axis=1, keepdims=True)
        weighted = keys.astype(F32) * jnp.exp(upright(log_in) - top)
        local[h, 0:qk, :] = dot(weighted.astype(BF16), values, ((0,), (0,)))
        normal = jnp.sum(weighted, axis=0, keepdims=True)
        local[h, qk : qk + 8, 0:qk] = jnp.broadcast_to(normal, (8, qk))
        decay = cum_ref[pl.ds(h, 1), :][:, length - 1 : length]
        local[h, qk + 8 : qk + 16, :] = jnp.broadcast_to(top + decay, (8, vw))
        return carry

    with scope("summarise"):
        lax.fori_loop(0, head_count, summarise, 0)

    @pl.when(me == 0)
    def _():
        st_in[:, 0 : qk + 8, :] = jnp.zeros((head_count, qk + 8, vw), F32)
        st_in[:, qk + 8 : qk + 16, :] = jnp.full((head_count, 8, vw), LOG_FLOOR, F32)

    def carry_on(h, carry):
        @pl.when(me > 0)
        def _():
            with scope("chainwait"):
                chain(h).wait_recv()

        decay = cum_ref[pl.ds(h, 1), :][:, length - 1 : length]
        carried_max = st_in[h, qk + 8 : qk + 9, :] + decay
        own_max = local[h, qk + 8 : qk + 9, :]
        new_max = jnp.maximum(carried_max, own_max)
        keep = jnp.exp(carried_max - new_max)
        add = jnp.exp(own_max - new_max)
        st_out[h, 0:qk, :] = keep * st_in[h, 0:qk, :] + add * local[h, 0:qk, :]
        st_out[h, qk : qk + 8, 0:qk] = (
            keep[:, 0:qk] * st_in[h, qk : qk + 8, 0:qk]
            + add[:, 0:qk] * local[h, qk : qk + 8, 0:qk]
        )
        st_out[h, qk : qk + 8, qk:vw] = jnp.zeros((8, vw - qk), F32)
        st_out[h, qk + 8 : qk + 16, :] = jnp.broadcast_to(new_max, (8, vw))

        @pl.when(me < ep - 1)
        def _():
            chain(h).start()

        return carry

    def heads(h, carry):
        columns = block(h, vw)
        queries = q_ref[:, block(h, qk)]
        keys = k_ref[:, block(h, qk)]
        scale = qk**-0.5
        causal = lax.broadcasted_iota(jnp.int32, (length, length), 1) <= lax.broadcasted_iota(
            jnp.int32, (length, length), 0
        )
        log_in = jnp.where(causal, a_ref[pl.ds(h, 1), :], -jnp.inf)
        prior_max = st_in[h, qk + 8 : qk + 9, 0:1]
        top = jnp.maximum(prior_max, jnp.max(log_in, axis=1, keepdims=True))
        scores = dot(queries, keys, ((1,), (1,))) * scale * jnp.exp(log_in - top)
        carried = jnp.exp(prior_max - top) * scale
        memory = st_in[h, 0:qk, :]
        high = memory.astype(BF16)
        low = (memory - high.astype(F32)).astype(BF16)
        numerator = carried * (dot(queries, high) + dot(queries, low)) + dot(
            scores.astype(BF16), v_ref[:, columns]
        )
        normal = st_in[h, qk : qk + 1, 0:qk]
        denominator = carried * jnp.sum(
            queries.astype(F32) * normal, axis=1, keepdims=True
        ) + jnp.sum(scores, axis=1, keepdims=True)
        floor = jnp.exp(-(upright(cum_ref[pl.ds(h, 1), :]) + top))
        value = numerator / jnp.maximum(jnp.abs(denominator), floor)
        value = value * lax.rsqrt(jnp.mean(value * value, axis=1, keepdims=True) + EPSILON)
        gate = jax.nn.sigmoid(og_ref[:, columns].astype(F32))
        hm[0, :, columns] = (value * gain_ref[:, columns] * gate).astype(BF16)
        return carry

    for at in range(8, 14):
        loads[at].wait()

    with scope("routes"):
        settled(rall.at[pl.ds(0, ep - 1)], route_recv.at[0]).wait_recv()
    wanted = jnp.zeros((ep, tokens), F32) + me.astype(F32)
    named = (rall[:, 0, :] == wanted) | (rall[:, 1, :] == wanted)
    ahead = dot(jnp.where(named, one, none).astype(BF16), strict)
    pos_ref[...] = jnp.where(named, ahead, -one)

    def when_between(step, low, high):
        return pl.when((step >= low) & (step <= high))

    quarter = me // (ep // 4)
    slot = (quarter + 2 * jnp.minimum(quarter, 1)) * (ep // 8)
    first_part = last

    def absorb(group, carry):
        @pl.when(group == 0)
        def _():
            take_own()

        @pl.when(group == 1)
        def _():
            take_partner()

        @when_between(group, 2, last - 1)
        def _():
            collect_group(group)

        @pl.when(group == last)
        def _():
            take_wide()

        with scope("expand"):
            expand(group)
        return carry

    def pass_share(group, carry):
        relay_share(group)
        return carry

    def finish_group(group, carry):
        contract(group)
        return carry

    def relay_heads(part):
        if square:
            for j in direct:
                with scope("HR"):
                    head_spread(part, j, 0).wait_recv()
                head_onward(part, j).start()

    def settle():
        settled(rall.at[pl.ds(0, ep - 1)], sent.at[0]).wait_send()
        settled(full.at[0, pl.ds(1, len(direct))], sent.at[1]).wait_send()
        settled(full.at[1], sent.at[3]).wait_send()

        @pl.when(parity == 0)
        def _():
            settled(afull.at[pl.ds(1, tp - 1)], sent.at[4]).wait_send()
            settled(afull.at[pl.ds(1, tp - 1)], sent.at[5]).wait_send()

        for distance in range(ep // 2):
            below, above = me - 2 * distance, me + 2 * distance
            own = distance == 0

            @pl.when((below >= 0) & (me < ep - 2))
            def _():
                z_copy(below, me + 2, up_send, own).wait_send()

            @pl.when((above < ep) & (me >= 2))
            def _():
                z_copy(above, me - 2, down_send, own).wait_send()

            if not own:

                @pl.when(below >= 0)
                def _():
                    z_copy(below, flip(me, 1), side_send).wait_send()

                @pl.when(above < ep)
                def _():
                    z_copy(above, flip(me, 1), side_send).wait_send()

        spread_rows = pl.ds(0, (ep - 3) * span)
        settled(tok.at[many, spread_rows], sent.at[6]).wait_send()
        settled(hid.at[many], sent.at[8]).wait_send()
        if square:
            settled(full.at[0, 3], sent.at[2]).wait_send()
            settled(tok.at[0, spread_rows], sent.at[7]).wait_send()
            settled(hid.at[0], sent.at[9]).wait_send()

        @pl.when(me < ep - 1)
        def _():
            settled(st_out, sent.at[13]).wait_send()

    def combine():
        returns = pl.ds(0, (ep - 1) * span)
        with scope("retwait"):
            settled(ret.at[returns], ret_recv.at[0]).wait_recv()
        ret[0:span, :] = outb[0:span, :]
        places = lax.broadcasted_iota(jnp.int32, (ret.shape[0], tokens), 0).astype(F32)
        total = jnp.zeros((tokens, width), F32)
        for route in range(weight_ref.shape[0]):
            hit = places == slot_row_ref[route : route + 1, :]
            picked = dot(hit.astype(F32).astype(BF16), ret[...], ((0,), (0,)))
            total += picked * upright(weight_ref[route : route + 1, :])
        exp_ref[...] = total.astype(BF16)
        settled(ret.at[returns], sent.at[10]).wait_send()

    def mix(part):
        rows = block(part, tile)
        with scope("M"):
            if not square:
                for j in direct:
                    head_spread(part, j, 0).wait_recv()
            settled(hm.at[many, piece(0, 0, tile_half)], head_rest.at[part]).wait_recv()

        def share_of(j):
            inputs = pl.ds(pl.multiple_of(flip(mine, j) * width, width), width)
            return dot(hm[j, rows, :], wm_ref[inputs, :])

        total = jnp.zeros((tile, width), F32)
        for j in range(tp - 1):
            total += share_of(j)
        partial[...] = total
        if square:
            with scope("M2"):
                settled(hm.at[3, rows], hfwd_recv.at[part]).wait_recv()
        mix_ref[rows, :] = (partial[...] + share_of(tp - 1)).astype(BF16)

    def step(k, carry):
        @pl.when(k == slot)
        def _():
            with scope("chain"):
                lax.fori_loop(0, head_count, carry_on, 0)
            with scope("heads"):
                lax.fori_loop(0, head_count // 2, heads, 0)

        @pl.when(k == slot + 1)
        def _():
            with scope("heads"):
                lax.fori_loop(head_count // 2, head_count, heads, 0)

        @pl.when(k == 0)
        def _():
            relay_own()

        @when_between(k, 2, last + 1)
        def _():
            lax.fori_loop(jnp.where(k == 2, 0, k - 1), k, absorb, 0)

        @when_between(k, 2, last - 1)
        def _():
            relay_group(k)

        @when_between(k, first_part, first_part + PARTS - 1)
        def _():
            relay_heads(k - first_part)

        @when_between(k, 3, last + 2)
        def _():
            lax.fori_loop(jnp.where(k == 3, 0, k - 2), k - 1, finish_group, 0)

        @when_between(k, 1, last - 2)
        def _():
            send_group(k + 1)

        @when_between(k, first_part - 1, first_part + PARTS - 2)
        def _():
            for j in direct:
                head_spread(k + 1 - first_part, j, 0).start()

        @when_between(k, 2, last + 1)
        def _():
            lax.fori_loop(jnp.where(k == 2, 0, k - 1), k, pass_share, 0)

        @when_between(k, 1, last - 2)
        def _():
            for j in direct:
                spread(k + 1, j, 1).start()

        @when_between(k, first_part - 1, first_part + PARTS - 2)
        def _():
            for j in direct:
                head_spread(k + 1 - first_part, j, 1).start()

        @pl.when((k == 2) & (parity == 0))
        def _():
            for j in range(1, tp):
                wide_copy(j, flip(me, 2), True).start()

        @pl.when((k == last - 1) & (parity == 0))
        def _():
            for j in range(1, tp):
                with scope("A"):
                    wide_copy(j, me, False).wait_recv()
                wide_copy(j, flip(me, 1), False).start()

        @pl.when(k == first_part + PARTS)
        def _():
            settle()
            combine()

        @pl.when(k > first_part)
        def _():
            mix(k - first_part - 1)

        return carry

    lax.fori_loop(0, first_part + PARTS + 1, step, 0)

    with scope("fin"):
        settled(hm.at[many], sent.at[11]).wait_send()
        if square:
            settled(hm.at[0], sent.at[12]).wait_send()


def body(
    query_rows,
    key_rows,
    value_rows,
    in_gate,
    forget_gate,
    out_gate,
    head_gain,
    mix_weight,
    expert_input,
    routes,
    route_weight,
    gate_weight,
    up_weight,
    down_weight,
):
    ep, tp = lax.axis_size("ep"), lax.axis_size("tp")
    head_count, length = in_gate.shape
    token_count, fanout = routes.shape
    width = expert_input.shape[1]
    units = gate_weight.shape[1]
    capacity = 2 * token_count * fanout // ep
    slot_count = ep * capacity
    qk = query_rows.shape[1] // head_count
    vw = value_rows.shape[1] // head_count

    vmem = pl.BlockSpec(memory_space=pltpu.VMEM)
    anywhere = pl.BlockSpec(memory_space=pl.ANY)
    dma = pltpu.SemaphoreType.DMA
    gate_local, up_local, down_local = gate_weight[0], up_weight[0], down_weight[0]
    small = (expert_input, routes.T, route_weight.T, in_gate, forget_gate, head_gain[None, :])
    big = (query_rows, key_rows, value_rows, out_gate, gate_local, up_local, down_local, mix_weight)
    state = (head_count, qk + PAD, vw)
    direct = 2 if tp == 4 else tp - 1
    return pl.pallas_call(
        functools.partial(kernel, ep, tp, head_count, mix_weight.shape[0]),
        out_shape=(
            pltpu.VMEM((length, width), BF16),
            pltpu.VMEM((token_count, width), BF16),
        ),
        in_specs=[anywhere] * 14,
        out_specs=(vmem, vmem),
        scratch_shapes=[pltpu.VMEM(array.shape, array.dtype) for array in small + big]
        + [
            pltpu.VMEM((head_count, length), F32),
            pltpu.VMEM((head_count, length), F32),
            pltpu.VMEM((fanout, token_count), F32),
            pltpu.VMEM((ep, token_count), F32),
            pltpu.VMEM((8, token_count), F32),
            pltpu.VMEM((ep, 8, token_count), F32),
            pltpu.VMEM((2, tp, token_count, width), BF16),
            pltpu.VMEM((ep, token_count, width), BF16),
            pltpu.VMEM((tp, token_count, width), BF16),
            pltpu.VMEM((tp, slot_count, width), BF16),
            pltpu.VMEM((tp, slot_count, units), BF16),
            pltpu.VMEM((slot_count, width), BF16),
            pltpu.VMEM((slot_count, width), BF16),
            pltpu.VMEM((tp, length, width), BF16),
            pltpu.VMEM(state, F32),
            pltpu.VMEM(state, F32),
            pltpu.VMEM(state, F32),
            pltpu.VMEM((length // PARTS, width), F32),
            dma((14,)),
            dma((14,)),
            dma((1,)),
            dma((direct, 2)),
            dma((2,)),
            dma((tp,)),
            dma((ep,)),
            dma((ep,)),
            dma((ep,)),
            dma((ep,)),
            dma((tp,)),
            dma((ep - 3, direct)),
            dma((ep - 3,)),
            dma((ep - 3,)),
            dma((ep, direct)),
            dma((ep,)),
            dma((1,)),
            dma((PARTS, direct)),
            dma((PARTS,)),
            dma((PARTS,)),
            dma((head_count,)),
        ],
        compiler_params=pltpu.CompilerParams(
            collective_id=0, has_side_effects=True, vmem_limit_bytes=58000 * 1024
        ),
    )(
        *small,
        *big,
    )


def solution(mesh):
    in_specs = (
        P("ep", "tp"),
        P("ep", "tp"),
        P("ep", "tp"),
        P("tp", "ep"),
        P("tp", "ep"),
        P("ep", "tp"),
        P("tp"),
        P(None, "tp"),
        P("ep", "tp"),
        P("ep", None),
        P("ep", None),
        P("ep", "tp", None),
        P("ep", "tp", None),
        P("ep", None, "tp"),
    )
    out_specs = (P("ep", "tp"), P("ep", "tp"))
    return jax.shard_map(body, mesh=mesh, in_specs=in_specs, out_specs=out_specs, check_vma=False)
```

```python
import functools

import jax
import jax.numpy as jnp
from jax import lax
from jax.experimental import pallas as pl
from jax.experimental.pallas import tpu as pltpu
from jax.sharding import PartitionSpec as P

EPSILON = 1e-06
LOG_FLOOR = -1e30
F32 = jnp.float32
BF16 = jnp.bfloat16
PARTS = 4
PAD = 16


def flip(index, bits):
    place = 1
    while place <= bits:
        if bits & place:
            index = index + place * (1 - 2 * ((index // place) % 2))
        place *= 2
    return index


def flip_by(index, bits, size):
    place = 1
    while place < size:
        index = index + ((bits // place) % 2) * place * (1 - 2 * ((index // place) % 2))
        place *= 2
    return index


def dot(left, right, contract=((1,), (0,))):
    return lax.dot_general(left, right, (contract, ((), ())), preferred_element_type=F32)


def upright(row):
    size = row.shape[1]
    own = lax.broadcasted_iota(jnp.int32, (size, size), 0) == lax.broadcasted_iota(
        jnp.int32, (size, size), 1
    )
    return jnp.sum(jnp.where(own, row, jnp.zeros((), row.dtype)), axis=1, keepdims=True)


def scope(name):
    return jax.named_scope(name)


def kernel(
    ep,
    tp,
    head_count,
    model_width,
    x_hbm,
    routes_hbm,
    weight_hbm,
    in_hbm,
    forget_hbm,
    gain_hbm,
    q_hbm,
    k_hbm,
    v_hbm,
    og_hbm,
    wg_hbm,
    wu_hbm,
    wd_hbm,
    wm_hbm,
    mix_ref,
    exp_ref,
    x_ref,
    routes_ref,
    weight_ref,
    in_ref,
    forget_ref,
    gain_ref,
    q_ref,
    k_ref,
    v_ref,
    og_ref,
    wg_ref,
    wu_ref,
    wd_ref,
    wm_ref,
    a_ref,
    cum_ref,
    slot_row_ref,
    pos_ref,
    named_ref,
    rall,
    full,
    zraw,
    afull,
    corner,
    tok,
    hid,
    outb,
    ret,
    hm,
    local,
    st_in,
    st_out,
    partial,
    load_sem,
    sent,
    route_recv,
    own_recv,
    ownf_recv,
    part_recv,
    z_send,
    side_send,
    z_recv,
    a_recv,
    b_recv,
    tok_recv,
    tok_rest,
    fwd_recv,
    hid_recv,
    hidf_recv,
    ret_recv,
    head_recv,
    head_rest,
    hfwd_recv,
    st_recv,
):
    me = lax.axis_index("ep")
    mine = lax.axis_index("tp")
    span = outb.shape[0] // ep
    width = x_ref.shape[1]
    length = q_ref.shape[0]
    qk = q_ref.shape[1] // head_count
    vw = v_ref.shape[1] // head_count
    units = wg_ref.shape[0]
    square = tp == 4
    direct = (1, 2) if square else tuple(range(1, tp))

    loads = [
        pltpu.make_async_copy(source, target, load_sem.at[at])
        for at, (source, target) in enumerate(
            [
                (x_hbm, x_ref),
                (routes_hbm, routes_ref),
                (forget_hbm, forget_ref),
                (in_hbm, in_ref),
                (weight_hbm, weight_ref),
                (gain_hbm, gain_ref),
                (k_hbm, k_ref),
                (v_hbm, v_ref),
                (q_hbm, q_ref),
                (og_hbm, og_ref),
                (wg_hbm, wg_ref),
                (wu_hbm, wu_ref),
                (wd_hbm, wd_ref),
                (wm_hbm, wm_ref),
            ]
        )
    ]
    barrier = pltpu.get_barrier_semaphore()
    for i in range(1, ep):
        pl.semaphore_signal(barrier, inc=1, device_id={"ep": flip(me, i)})
    for j in range(1, tp):
        pl.semaphore_signal(barrier, inc=1, device_id={"tp": flip(mine, j)})

    for load in loads:
        load.start()

    tokens = x_ref.shape[0]

    def block(at, size):
        return pl.ds(pl.multiple_of(at * size, size), size)

    def settled(ref, sem):
        return pltpu.make_async_remote_copy(ref, ref, sem, sem, device_id={"tp": flip(mine, 1)})

    def route_copy(i):
        return pltpu.make_async_remote_copy(
            named_ref,
            rall.at[me],
            sent.at[0],
            route_recv.at[0],
            device_id={"ep": flip(me, i)},
        )

    def own_spread(j, part):
        rows = pl.ds(part * (tokens // 2), tokens // 2)
        return pltpu.make_async_remote_copy(
            x_ref.at[rows],
            full.at[0, j, rows],
            sent.at[1],
            own_recv.at[j - 1, part],
            device_id={"tp": flip(mine, j)},
        )

    def own_onward(j):
        size = tokens // 2
        part = pl.ds((j - 1) * size, size)
        return pltpu.make_async_remote_copy(
            full.at[0, j, part],
            full.at[0, 3, part],
            sent.at[2],
            ownf_recv.at[j - 1],
            device_id={"tp": flip(mine, 3 - j)},
        )

    def to_partner(j):
        return pltpu.make_async_remote_copy(
            full.at[0, j] if j else x_ref,
            full.at[1, j],
            sent.at[3],
            part_recv.at[j],
            device_id={"ep": flip(me, 1)},
        )

    def z_copy(source, target, part):
        rows = pl.ds(part * (tokens // 2), tokens // 2)
        return pltpu.make_async_remote_copy(
            zraw.at[source, rows],
            zraw.at[source, rows],
            z_send.at[source, part],
            z_recv.at[source, part],
            device_id={"ep": target},
        )

    def z_own(target, part, sem):
        rows = pl.ds(part * (tokens // 2), tokens // 2)
        return pltpu.make_async_remote_copy(
            x_ref.at[rows],
            zraw.at[me, rows],
            sem,
            z_recv.at[me, part],
            device_id={"ep": target},
        )

    def z_side(source, target):
        return pltpu.make_async_remote_copy(
            zraw.at[source],
            zraw.at[source],
            side_send.at[source],
            z_recv.at[source, 0],
            device_id={"ep": target},
        )

    parity = me % 2
    last = ep - 1
    spare = flip(me - parity, 2)
    other = spare + 1

    def wide_copy(j, target, start_full):
        return pltpu.make_async_remote_copy(
            full.at[0, j] if start_full else afull.at[j],
            afull.at[j],
            sent.at[4 if start_full else 5],
            a_recv.at[j],
            device_id={"ep": target},
        )

    def corner_copy(target, start_full):
        return pltpu.make_async_remote_copy(
            full.at[0, 3] if start_full else corner,
            corner,
            sent.at[14 if start_full else 15],
            b_recv.at[0],
            device_id={"ep": target},
        )

    def index_of(place):
        middle = jnp.where(place == 2, 3 - parity, place + 1)
        return jnp.where(place < 2, place, jnp.where(place == last, 2 + parity, middle))

    loads[0].wait()
    loads[1].wait()
    routes = routes_ref[...].astype(F32)
    named_ref[0:2, :] = routes
    named_ref[2:8, :] = jnp.full((6, tokens), -1.0, F32)
    full[0, 0] = x_ref[...]
    with scope("barrier"):
        pl.semaphore_wait(barrier, ep - 1 + tp - 1)

    for step in range(2):
        for j in direct:
            own_spread(j, (j - 1 + step) % 2).start()
    for i in range(1, ep):
        route_copy(i).start()

    for part in range(2):

        @pl.when(me < ep - 2)
        def _():
            z_own(me + 2, part, sent.at[16]).start()

        @pl.when(me >= 2)
        def _():
            z_own(me - 2, part, sent.at[17]).start()

    to_partner(0).start()
    rall[me] = named_ref[...]

    half = span // 2

    def piece(start, at, size):
        return pl.ds(pl.multiple_of(start + at * size, size), size)

    def spread(group, j, turn):
        rows = piece(group * span, (j - 1 + turn) % 2, half)
        return pltpu.make_async_remote_copy(
            tok.at[0, rows],
            tok.at[j, rows],
            sent.at[6],
            tok_rest.at[group - 2] if turn else tok_recv.at[group - 2, j - 1],
            device_id={"tp": flip(mine, j)},
        )

    def onward(group, j):
        part = piece(group * span, j - 1, half)
        return pltpu.make_async_remote_copy(
            tok.at[j, part],
            tok.at[3, part],
            sent.at[7],
            fwd_recv.at[group - 2],
            device_id={"tp": flip(mine, 3 - j)},
        )

    def share(group, j):
        return pltpu.make_async_remote_copy(
            hid.at[0, block(group, span)],
            hid.at[j, block(group, span)],
            sent.at[8],
            hid_recv.at[group, j - 1],
            device_id={"tp": flip(mine, j)},
        )

    def share_onward(group, j):
        part = piece(group * span, j - 1, half)
        return pltpu.make_async_remote_copy(
            hid.at[j, part],
            hid.at[3, part],
            sent.at[9],
            hidf_recv.at[group],
            device_id={"tp": flip(mine, 3 - j)},
        )

    def give_back(place, i):
        return pltpu.make_async_remote_copy(
            outb.at[block(place, span)],
            ret.at[block(i, span)],
            sent.at[10],
            ret_recv.at[0],
            device_id={"ep": flip_by(me, i, ep)},
        )

    tile = length // PARTS
    tile_half = tile // 2

    def head_spread(part, j, turn):
        rows = piece(part * tile, (j - 1 + turn) % 2, tile_half)
        return pltpu.make_async_remote_copy(
            hm.at[0, rows],
            hm.at[j, rows],
            sent.at[11],
            head_rest.at[part] if turn else head_recv.at[part, j - 1],
            device_id={"tp": flip(mine, j)},
        )

    def head_onward(part, j):
        rows = piece(part * tile, j - 1, tile_half)
        return pltpu.make_async_remote_copy(
            hm.at[j, rows],
            hm.at[3, rows],
            sent.at[12],
            hfwd_recv.at[part],
            device_id={"tp": flip(mine, 3 - j)},
        )

    def chain(h):
        return pltpu.make_async_remote_copy(
            st_out.at[h],
            st_in.at[h],
            sent.at[13],
            st_recv.at[h],
            device_id={"ep": me + 1},
        )

    many = pl.ds(0, len(direct))

    def pass_along(distance, part):
        below, above = me - 2 * distance, me + 2 * distance

        @pl.when(below >= 0)
        def _():
            with scope("F"):
                z_copy(below, me, part).wait_recv()

            @pl.when(me < ep - 2)
            def _():
                z_copy(below, me + 2, part).start()

            if part:
                z_side(below, flip(me, 1)).start()

        @pl.when(above < ep)
        def _():
            with scope("F"):
                z_copy(above, me, part).wait_recv()

            @pl.when(me >= 2)
            def _():
                z_copy(above, me - 2, part).start()

            if part:
                z_side(above, flip(me, 1)).start()

    def choose(source, rows):
        places = lax.broadcasted_iota(jnp.int32, (span, tokens), 0).astype(F32)
        hit = places == pos_ref[pl.ds(source, 1), :]
        return dot(hit.astype(F32).astype(BF16), rows).astype(BF16)

    def send_group(group):
        index = index_of(group)
        source = flip_by(me, index, ep)

        @pl.when(group == 2)
        def _():
            pass_along(1, 1)

        @pl.when((group > 2) & (index % 2 == 0))
        def _():
            pass_along(index // 2, 0)
            pass_along(index // 2, 1)

        @pl.when(index % 2 == 1)
        def _():
            with scope("S"):
                z_side(source, me).wait_recv()

        tok[0, block(group, span), :] = choose(source, zraw[source])
        for j in direct:
            spread(group, j, 0).start()

    def relay_own():
        for j in direct:
            with scope("O"):
                own_spread(j, (j - 1) % 2).wait_recv()
            if square:
                own_onward(j).start()
        pass_along(1, 0)
        for j in direct:
            with scope("O"):
                own_spread(j, j % 2).wait_recv()
            to_partner(j).start()

    def take_own():
        if square:
            with scope("O"):
                for j in direct:
                    own_onward(j).wait_recv()
            to_partner(3).start()
        for j in range(tp):
            tok[j, 0:span, :] = choose(me, full[0, j])

    def take_wide():
        @pl.when(parity == 1)
        def _():
            with scope("A"):
                z_side(spare, me).wait_recv()
                for j in range(1, tp):
                    wide_copy(j, me, False).wait_recv()

        rows = block(last, span)
        tok[0, rows, :] = choose(spare, zraw[spare])
        for j in range(1, tp):
            tok[j, rows, :] = choose(spare, afull[j])

    def take_partner():
        with scope("P"):
            for j in range(tp):
                to_partner(j).wait_recv()
        for j in range(tp):
            tok[j, span : 2 * span, :] = choose(flip(me, 1), full[1, j])

    def relay_group(group):
        if square:
            for j in direct:
                with scope("R"):
                    spread(group, j, 0).wait_recv()
                onward(group, j).start()

    def full_relay(group):
        rows = block(group, span)

        @pl.when(group > 2)
        def _():
            settled(tok.at[3, rows], fwd_recv.at[group - 2]).wait_recv()

        @pl.when(group == 2)
        def _():
            for j in direct:
                spread(group, j, 0).wait_recv()

            @pl.when(parity == 0)
            def _():
                corner_copy(me, False).wait_recv()

            tok[3, rows, :] = choose(other, corner[...])

    def collect_group(group):
        with scope("C"):
            if square:
                full_relay(group)
            else:
                for j in direct:
                    spread(group, j, 0).wait_recv()
            settled(tok.at[many, piece(0, 0, half)], tok_rest.at[group - 2]).wait_recv()

    def relay_share(group):
        if square:
            for j in direct:
                with scope("Q"):
                    share(group, j).wait_recv()
                share_onward(group, j).start()

    def expand(group):
        rows = block(group, span)
        gate = jnp.zeros((span, units), F32)
        up = jnp.zeros((span, units), F32)
        squares = jnp.zeros((span, 1), F32)
        for j in range(tp):
            piece = tok[j, rows, :]
            columns = pl.ds(pl.multiple_of(flip(mine, j) * width, width), width)
            gate += dot(piece, wg_ref[:, columns], ((1,), (1,)))
            up += dot(piece, wu_ref[:, columns], ((1,), (1,)))
            wide = piece.astype(F32)
            squares += jnp.sum(wide * wide, axis=1, keepdims=True)
        inverse = lax.rsqrt(squares / model_width + EPSILON)
        hid[0, rows, :] = (jax.nn.silu(gate * inverse) * (up * inverse)).astype(BF16)
        for j in direct:
            share(group, j).start()

    def contract(group):
        rows = block(group, span)
        with scope("K"):
            if square:
                settled(hid.at[3, block(group, span)], hidf_recv.at[group]).wait_recv()
            else:
                for j in direct:
                    share(group, j).wait_recv()
        total = jnp.zeros((span, width), F32)
        for j in range(tp):
            at = pl.ds(pl.multiple_of(flip(mine, j) * units, units), units)
            total += dot(hid[j, rows, :], wd_ref[at, :])
        outb[rows, :] = total.astype(BF16)

        @pl.when(group > 0)
        def _():
            give_back(group, index_of(group)).start()

    for at in range(2, 6):
        loads[at].wait()
    forget = forget_ref[...]
    decay_log = jnp.minimum(forget, 0.0) - jnp.log1p(jnp.exp(-jnp.abs(forget)))
    head_part = decay_log.astype(BF16)
    rest = decay_log - head_part.astype(F32)
    mid_part = rest.astype(BF16)
    low_part = (rest - mid_part.astype(F32)).astype(BF16)
    upper = lax.broadcasted_iota(jnp.int32, (length, length), 0) <= lax.broadcasted_iota(
        jnp.int32, (length, length), 1
    )
    upper = upper.astype(F32).astype(BF16)
    cumulative = dot(head_part, upper) + dot(mid_part, upper) + dot(low_part, upper)
    cum_ref[...] = cumulative
    a_ref[...] = in_ref[...] - cumulative

    strict = lax.broadcasted_iota(jnp.int32, (tokens, tokens), 0) < lax.broadcasted_iota(
        jnp.int32, (tokens, tokens), 1
    )
    strict = strict.astype(F32).astype(BF16)
    order = lax.broadcasted_iota(jnp.int32, (ep, tokens), 0)
    experts = (order ^ me).astype(F32)
    one = jnp.ones((ep, tokens), F32)
    none = jnp.zeros((ep, tokens), F32)
    first = jnp.where(experts == routes[0:1, :], one, none)
    second = jnp.where(experts == routes[1:2, :], one, none)
    places = (order * span).astype(F32) + dot((first + second).astype(BF16), strict)
    slot_row_ref[0:1, :] = jnp.sum(first * places, axis=0, keepdims=True)
    slot_row_ref[1:2, :] = jnp.sum(second * places, axis=0, keepdims=True)

    loads[6].wait()
    loads[7].wait()

    def summarise(h, carry):
        keys = k_ref[:, block(h, qk)]
        values = v_ref[:, block(h, vw)]
        log_in = a_ref[pl.ds(h, 1), :]
        top = jnp.max(log_in, axis=1, keepdims=True)
        weighted = keys.astype(F32) * jnp.exp(upright(log_in) - top)
        local[h, 0:qk, :] = dot(weighted.astype(BF16), values, ((0,), (0,)))
        normal = jnp.sum(weighted, axis=0, keepdims=True)
        local[h, qk : qk + 8, 0:qk] = jnp.broadcast_to(normal, (8, qk))
        decay = cum_ref[pl.ds(h, 1), :][:, length - 1 : length]
        local[h, qk + 8 : qk + 16, :] = jnp.broadcast_to(top + decay, (8, vw))
        return carry

    with scope("summarise"):
        lax.fori_loop(0, head_count, summarise, 0)

    @pl.when(me == 0)
    def _():
        st_in[:, 0 : qk + 8, :] = jnp.zeros((head_count, qk + 8, vw), F32)
        st_in[:, qk + 8 : qk + 16, :] = jnp.full((head_count, 8, vw), LOG_FLOOR, F32)

    def carry_on(h, carry):
        @pl.when(me > 0)
        def _():
            with scope("chainwait"):
                chain(h).wait_recv()

        decay = cum_ref[pl.ds(h, 1), :][:, length - 1 : length]
        carried_max = st_in[h, qk + 8 : qk + 9, :] + decay
        own_max = local[h, qk + 8 : qk + 9, :]
        new_max = jnp.maximum(carried_max, own_max)
        keep = jnp.exp(carried_max - new_max)
        add = jnp.exp(own_max - new_max)
        st_out[h, 0:qk, :] = keep * st_in[h, 0:qk, :] + add * local[h, 0:qk, :]
        st_out[h, qk : qk + 8, 0:qk] = (
            keep[:, 0:qk] * st_in[h, qk : qk + 8, 0:qk]
            + add[:, 0:qk] * local[h, qk : qk + 8, 0:qk]
        )
        st_out[h, qk : qk + 8, qk:vw] = jnp.zeros((8, vw - qk), F32)
        st_out[h, qk + 8 : qk + 16, :] = jnp.broadcast_to(new_max, (8, vw))

        @pl.when(me < ep - 1)
        def _():
            chain(h).start()

        return carry

    def heads(h, carry):
        columns = block(h, vw)
        queries = q_ref[:, block(h, qk)]
        keys = k_ref[:, block(h, qk)]
        scale = qk**-0.5
        causal = lax.broadcasted_iota(jnp.int32, (length, length), 1) <= lax.broadcasted_iota(
            jnp.int32, (length, length), 0
        )
        log_in = jnp.where(causal, a_ref[pl.ds(h, 1), :], -jnp.inf)
        prior_max = st_in[h, qk + 8 : qk + 9, 0:1]
        top = jnp.maximum(prior_max, jnp.max(log_in, axis=1, keepdims=True))
        scores = dot(queries, keys, ((1,), (1,))) * scale * jnp.exp(log_in - top)
        carried = jnp.exp(prior_max - top) * scale
        memory = st_in[h, 0:qk, :]
        high = memory.astype(BF16)
        low = (memory - high.astype(F32)).astype(BF16)
        numerator = carried * (dot(queries, high) + dot(queries, low)) + dot(
            scores.astype(BF16), v_ref[:, columns]
        )
        normal = st_in[h, qk : qk + 1, 0:qk]
        denominator = carried * jnp.sum(
            queries.astype(F32) * normal, axis=1, keepdims=True
        ) + jnp.sum(scores, axis=1, keepdims=True)
        floor = jnp.exp(-(upright(cum_ref[pl.ds(h, 1), :]) + top))
        value = numerator / jnp.maximum(jnp.abs(denominator), floor)
        value = value * lax.rsqrt(jnp.mean(value * value, axis=1, keepdims=True) + EPSILON)
        gate = jax.nn.sigmoid(og_ref[:, columns].astype(F32))
        hm[0, :, columns] = (value * gain_ref[:, columns] * gate).astype(BF16)
        return carry

    for at in range(8, 14):
        loads[at].wait()

    with scope("routes"):
        settled(rall.at[pl.ds(0, ep - 1)], route_recv.at[0]).wait_recv()
    wanted = jnp.zeros((ep, tokens), F32) + me.astype(F32)
    named = (rall[:, 0, :] == wanted) | (rall[:, 1, :] == wanted)
    ahead = dot(jnp.where(named, one, none).astype(BF16), strict)
    pos_ref[...] = jnp.where(named, ahead, -one)

    def when_between(step, low, high):
        return pl.when((step >= low) & (step <= high))

    quarter = me // (ep // 4)
    slot = quarter * (7 - quarter) // 2 * (ep // 8)
    first_part = last
    early = (1,) if square else direct
    late = (1 - (me // 2) % 2) * jnp.minimum(me // 2, 1)
    final = last + 1 + ((me // 2) % 2) * jnp.minimum(me // 4, 1)
    tardy = late * (1 - parity)

    def turn(n):
        return jnp.where(n < 2, n, jnp.where(n == last, n, jnp.where(n == last - 1, 2, n + 1)))

    def turns(k):
        low = jnp.where(k == 2, 0, jnp.where(k == final, last, k - 2))
        high = jnp.where(k == last, k, k - 1)
        return low, jnp.where(k == 2, 2, jnp.where(k == final, last + 1, high))

    def busy(k):
        return (k == 2) | ((k >= 4) & (k <= last)) | (k == final)

    def absorb(n, carry):
        group = turn(n)

        @pl.when(group == 0)
        def _():
            take_own()

        @pl.when(group == 1)
        def _():
            take_partner()

        @when_between(group, 2, last - 1)
        def _():
            collect_group(group)

        @pl.when(group == last)
        def _():
            take_wide()

        with scope("expand"):
            expand(group)
        return carry

    def pass_share(n, carry):
        relay_share(turn(n))
        return carry

    def finish_group(n, carry):
        contract(turn(n))
        return carry

    def relay_heads(part):
        if square:
            for j in direct:
                with scope("HR"):
                    head_spread(part, j, 0).wait_recv()
                head_onward(part, j).start()

    def settle():
        settled(rall.at[pl.ds(0, ep - 1)], sent.at[0]).wait_send()
        settled(full.at[0, pl.ds(1, len(direct))], sent.at[1]).wait_send()
        settled(full.at[1], sent.at[3]).wait_send()

        @pl.when(parity == 0)
        def _():
            settled(afull.at[pl.ds(1, tp - 1)], sent.at[4]).wait_send()
            settled(afull.at[pl.ds(1, tp - 1)], sent.at[5]).wait_send()

        @pl.when(me < ep - 2)
        def _():
            settled(x_ref, sent.at[16]).wait_send()

        @pl.when(me >= 2)
        def _():
            settled(x_ref, sent.at[17]).wait_send()

        for distance in range(1, ep // 2):
            below, above = me - 2 * distance, me + 2 * distance

            @pl.when(below >= 0)
            def _():
                z_side(below, flip(me, 1)).wait_send()

                @pl.when(me < ep - 2)
                def _():
                    for part in range(2):
                        z_copy(below, me + 2, part).wait_send()

            @pl.when(above < ep)
            def _():
                z_side(above, flip(me, 1)).wait_send()

                @pl.when(me >= 2)
                def _():
                    for part in range(2):
                        z_copy(above, me - 2, part).wait_send()

        spread_rows = pl.ds(0, (ep - 3) * span)
        settled(tok.at[many, spread_rows], sent.at[6]).wait_send()
        settled(hid.at[many], sent.at[8]).wait_send()
        if square:
            settled(full.at[0, 3], sent.at[2]).wait_send()
            settled(tok.at[0, pl.ds(0, (ep - 4) * span)], sent.at[7]).wait_send()

            @pl.when(parity == 1)
            def _():
                settled(corner, sent.at[14]).wait_send()
                settled(corner, sent.at[15]).wait_send()

            settled(hid.at[0], sent.at[9]).wait_send()

        @pl.when(me < ep - 1)
        def _():
            settled(st_out, sent.at[13]).wait_send()

    def combine():
        returns = pl.ds(0, (ep - 1) * span)
        with scope("retwait"):
            settled(ret.at[returns], ret_recv.at[0]).wait_recv()
        ret[0:span, :] = outb[0:span, :]
        places = lax.broadcasted_iota(jnp.int32, (ret.shape[0], tokens), 0).astype(F32)
        total = jnp.zeros((tokens, width), F32)
        for route in range(weight_ref.shape[0]):
            hit = places == slot_row_ref[route : route + 1, :]
            picked = dot(hit.astype(F32).astype(BF16), ret[...], ((0,), (0,)))
            total += picked * upright(weight_ref[route : route + 1, :])
        exp_ref[...] = total.astype(BF16)
        settled(ret.at[returns], sent.at[10]).wait_send()

    def mix(part):
        rows = block(part, tile)
        with scope("M"):
            if not square:
                for j in direct:
                    head_spread(part, j, 0).wait_recv()
            settled(hm.at[many, piece(0, 0, tile_half)], head_rest.at[part]).wait_recv()

        def share_of(j):
            inputs = pl.ds(pl.multiple_of(flip(mine, j) * width, width), width)
            return dot(hm[j, rows, :], wm_ref[inputs, :])

        total = jnp.zeros((tile, width), F32)
        for j in range(tp - 1):
            total += share_of(j)
        partial[...] = total
        if square:
            with scope("M2"):
                settled(hm.at[3, rows], hfwd_recv.at[part]).wait_recv()
        mix_ref[rows, :] = (partial[...] + share_of(tp - 1)).astype(BF16)

    def step(k, carry):
        @pl.when(k == slot)
        def _():
            with scope("chain"):
                lax.fori_loop(0, head_count, carry_on, 0)
            with scope("heads"):
                lax.fori_loop(0, head_count // 2, heads, 0)

        @pl.when(k == jnp.minimum(slot + 1, last - 1))
        def _():
            with scope("heads"):
                lax.fori_loop(head_count // 2, head_count, heads, 0)

        @pl.when(k == 0)
        def _():
            relay_own()

        @pl.when(busy(k))
        def _():
            lax.fori_loop(*turns(k), absorb, 0)

        @when_between(k, 3 if square else 2, last - 1)
        def _():
            relay_group(k)

        @when_between(k, first_part, first_part + PARTS - 1)
        def _():
            relay_heads(k - first_part)

        @pl.when(busy(k - 1))
        def _():
            lax.fori_loop(*turns(k - 1), finish_group, 0)

        if square:

            @pl.when((k == final - 1) & (parity == 0))
            def _():
                for j in (2, 3):
                    with scope("A3"):
                        wide_copy(j, me, False).wait_recv()
                    wide_copy(j, flip(me, 1), False).start()

        @when_between(k, 1, last - 2)
        def _():
            send_group(k + 1)

        @when_between(k, first_part - 1, first_part + PARTS - 2)
        def _():
            for j in direct:
                head_spread(k + 1 - first_part, j, 0).start()

        @pl.when(busy(k))
        def _():
            lax.fori_loop(*turns(k), pass_share, 0)

        @when_between(k, 1, last - 2)
        def _():
            for j in direct:
                spread(k + 1, j, 1).start()

        @when_between(k, first_part - 1, first_part + PARTS - 2)
        def _():
            for j in direct:
                head_spread(k + 1 - first_part, j, 1).start()

        @pl.when((k == 2) & (parity == 0))
        def _():
            for j in early:
                wide_copy(j, flip(me, 2), True).start()

        if square:

            @pl.when((k == 2 + 3 * late) & (parity == 0))
            def _():
                for j in (2, 3):
                    wide_copy(j, flip(me, 2), True).start()

            @pl.when((k == 2) & (parity == 1))
            def _():
                corner_copy(flip(me, 2), True).start()

            @pl.when((k == last - 1) & (parity == 1))
            def _():
                with scope("B"):
                    corner_copy(me, False).wait_recv()
                corner_copy(flip(me, 1), False).start()

        @pl.when((k == last - 1) & (parity == 0))
        def _():
            for j in early:
                with scope("A"):
                    wide_copy(j, me, False).wait_recv()
                wide_copy(j, flip(me, 1), False).start()

        @pl.when(k == first_part + PARTS)
        def _():
            settle()

        @pl.when((k == first_part + PARTS) & (tardy == 0))
        def _():
            combine()

        @pl.when(k > first_part)
        def _():
            mix(k - first_part - 1)

        @pl.when((k == first_part + PARTS) & (tardy == 1))
        def _():
            combine()

        return carry

    lax.fori_loop(0, first_part + PARTS + 1, step, 0)

    with scope("fin"):
        settled(hm.at[many], sent.at[11]).wait_send()
        if square:
            settled(hm.at[0], sent.at[12]).wait_send()


def body(
    query_rows,
    key_rows,
    value_rows,
    in_gate,
    forget_gate,
    out_gate,
    head_gain,
    mix_weight,
    expert_input,
    routes,
    route_weight,
    gate_weight,
    up_weight,
    down_weight,
):
    ep, tp = lax.axis_size("ep"), lax.axis_size("tp")
    head_count, length = in_gate.shape
    token_count, fanout = routes.shape
    width = expert_input.shape[1]
    units = gate_weight.shape[1]
    capacity = 2 * token_count * fanout // ep
    slot_count = ep * capacity
    qk = query_rows.shape[1] // head_count
    vw = value_rows.shape[1] // head_count

    vmem = pl.BlockSpec(memory_space=pltpu.VMEM)
    anywhere = pl.BlockSpec(memory_space=pl.ANY)
    dma = pltpu.SemaphoreType.DMA
    gate_local, up_local, down_local = gate_weight[0], up_weight[0], down_weight[0]
    small = (expert_input, routes.T, route_weight.T, in_gate, forget_gate, head_gain[None, :])
    big = (query_rows, key_rows, value_rows, out_gate, gate_local, up_local, down_local, mix_weight)
    state = (head_count, qk + PAD, vw)
    direct = 2 if tp == 4 else tp - 1
    return pl.pallas_call(
        functools.partial(kernel, ep, tp, head_count, mix_weight.shape[0]),
        out_shape=(
            pltpu.VMEM((length, width), BF16),
            pltpu.VMEM((token_count, width), BF16),
        ),
        in_specs=[anywhere] * 14,
        out_specs=(vmem, vmem),
        scratch_shapes=[pltpu.VMEM(array.shape, array.dtype) for array in small + big]
        + [
            pltpu.VMEM((head_count, length), F32),
            pltpu.VMEM((head_count, length), F32),
            pltpu.VMEM((fanout, token_count), F32),
            pltpu.VMEM((ep, token_count), F32),
            pltpu.VMEM((8, token_count), F32),
            pltpu.VMEM((ep, 8, token_count), F32),
            pltpu.VMEM((2, tp, token_count, width), BF16),
            pltpu.VMEM((ep, token_count, width), BF16),
            pltpu.VMEM((tp, token_count, width), BF16),
            pltpu.VMEM((token_count, width), BF16),
            pltpu.VMEM((tp, slot_count, width), BF16),
            pltpu.VMEM((tp, slot_count, units), BF16),
            pltpu.VMEM((slot_count, width), BF16),
            pltpu.VMEM((slot_count, width), BF16),
            pltpu.VMEM((tp, length, width), BF16),
            pltpu.VMEM(state, F32),
            pltpu.VMEM(state, F32),
            pltpu.VMEM(state, F32),
            pltpu.VMEM((length // PARTS, width), F32),
            dma((14,)),
            dma((18,)),
            dma((1,)),
            dma((direct, 2)),
            dma((2,)),
            dma((tp,)),
            dma((ep, 2)),
            dma((ep,)),
            dma((ep, 2)),
            dma((tp,)),
            dma((1,)),
            dma((ep - 3, direct)),
            dma((ep - 3,)),
            dma((ep - 3,)),
            dma((ep, direct)),
            dma((ep,)),
            dma((1,)),
            dma((PARTS, direct)),
            dma((PARTS,)),
            dma((PARTS,)),
            dma((head_count,)),
        ],
        compiler_params=pltpu.CompilerParams(
            collective_id=0, has_side_effects=True, vmem_limit_bytes=58000 * 1024
        ),
    )(
        *small,
        *big,
    )


def solution(mesh):
    in_specs = (
        P("ep", "tp"),
        P("ep", "tp"),
        P("ep", "tp"),
        P("tp", "ep"),
        P("tp", "ep"),
        P("ep", "tp"),
        P("tp"),
        P(None, "tp"),
        P("ep", "tp"),
        P("ep", None),
        P("ep", None),
        P("ep", "tp", None),
        P("ep", "tp", None),
        P("ep", None, "tp"),
    )
    out_specs = (P("ep", "tp"), P("ep", "tp"))
    return jax.shard_map(body, mesh=mesh, in_specs=in_specs, out_specs=out_specs, check_vma=False)
```

```python
import functools

import jax
import jax.numpy as jnp
from jax import lax
from jax.experimental import pallas as pl
from jax.experimental.pallas import tpu as pltpu
from jax.sharding import PartitionSpec as P

EPSILON = 1e-06
LOG_FLOOR = -1e30
F32 = jnp.float32
BF16 = jnp.bfloat16
PARTS = 4
PAD = 16


def flip(index, bits):
    place = 1
    while place <= bits:
        if bits & place:
            index = index + place * (1 - 2 * ((index // place) % 2))
        place *= 2
    return index


def flip_by(index, bits, size):
    place = 1
    while place < size:
        index = index + ((bits // place) % 2) * place * (1 - 2 * ((index // place) % 2))
        place *= 2
    return index


def dot(left, right, contract=((1,), (0,))):
    return lax.dot_general(left, right, (contract, ((), ())), preferred_element_type=F32)


def upright(row):
    size = row.shape[1]
    own = lax.broadcasted_iota(jnp.int32, (size, size), 0) == lax.broadcasted_iota(
        jnp.int32, (size, size), 1
    )
    return jnp.sum(jnp.where(own, row, jnp.zeros((), row.dtype)), axis=1, keepdims=True)


def scope(name):
    return jax.named_scope(name)


def kernel(
    ep,
    tp,
    head_count,
    model_width,
    x_hbm,
    routes_hbm,
    weight_hbm,
    in_hbm,
    forget_hbm,
    gain_hbm,
    q_hbm,
    k_hbm,
    v_hbm,
    og_hbm,
    wg_hbm,
    wu_hbm,
    wd_hbm,
    wm_hbm,
    mix_ref,
    exp_ref,
    x_ref,
    routes_ref,
    weight_ref,
    in_ref,
    forget_ref,
    gain_ref,
    q_ref,
    k_ref,
    v_ref,
    og_ref,
    wg_ref,
    wu_ref,
    wd_ref,
    wm_ref,
    a_ref,
    cum_ref,
    slot_row_ref,
    pos_ref,
    named_ref,
    rall,
    full,
    zraw,
    afull,
    corner,
    tok,
    hid,
    outb,
    ret,
    hm,
    local,
    st_in,
    st_out,
    partial,
    load_sem,
    sent,
    route_recv,
    own_recv,
    ownf_recv,
    part_recv,
    z_send,
    side_send,
    z_recv,
    a_recv,
    b_recv,
    tok_recv,
    tok_rest,
    fwd_recv,
    hid_recv,
    hidf_recv,
    ret_recv,
    head_recv,
    head_rest,
    hfwd_recv,
    st_recv,
):
    me = lax.axis_index("ep")
    mine = lax.axis_index("tp")
    span = outb.shape[0] // ep
    width = x_ref.shape[1]
    length = q_ref.shape[0]
    qk = q_ref.shape[1] // head_count
    vw = v_ref.shape[1] // head_count
    units = wg_ref.shape[0]
    square = tp == 4
    direct = (1, 2) if square else tuple(range(1, tp))

    loads = [
        pltpu.make_async_copy(source, target, load_sem.at[at])
        for at, (source, target) in enumerate(
            [
                (x_hbm, x_ref),
                (routes_hbm, routes_ref),
                (forget_hbm, forget_ref),
                (in_hbm, in_ref),
                (weight_hbm, weight_ref),
                (gain_hbm, gain_ref),
                (k_hbm, k_ref),
                (v_hbm, v_ref),
                (q_hbm, q_ref),
                (og_hbm, og_ref),
                (wg_hbm, wg_ref),
                (wu_hbm, wu_ref),
                (wd_hbm, wd_ref),
                (wm_hbm, wm_ref),
            ]
        )
    ]
    barrier = pltpu.get_barrier_semaphore()
    for i in range(1, ep):
        pl.semaphore_signal(barrier, inc=1, device_id={"ep": flip(me, i)})
    for j in range(1, tp):
        pl.semaphore_signal(barrier, inc=1, device_id={"tp": flip(mine, j)})

    for load in loads:
        load.start()

    tokens = x_ref.shape[0]

    def block(at, size):
        return pl.ds(pl.multiple_of(at * size, size), size)

    def settled(ref, sem):
        return pltpu.make_async_remote_copy(ref, ref, sem, sem, device_id={"tp": flip(mine, 1)})

    def route_copy(i):
        return pltpu.make_async_remote_copy(
            named_ref,
            rall.at[me],
            sent.at[0],
            route_recv.at[0],
            device_id={"ep": flip(me, i)},
        )

    def own_spread(j, part):
        rows = pl.ds(part * (tokens // 2), tokens // 2)
        return pltpu.make_async_remote_copy(
            x_ref.at[rows],
            full.at[0, j, rows],
            sent.at[1],
            own_recv.at[j - 1, part],
            device_id={"tp": flip(mine, j)},
        )

    def own_onward(j):
        size = tokens // 2
        part = pl.ds((j - 1) * size, size)
        return pltpu.make_async_remote_copy(
            full.at[0, j, part],
            full.at[0, 3, part],
            sent.at[2],
            ownf_recv.at[j - 1],
            device_id={"tp": flip(mine, 3 - j)},
        )

    def to_partner(j):
        return pltpu.make_async_remote_copy(
            full.at[0, j] if j else x_ref,
            full.at[1, j],
            sent.at[3],
            part_recv.at[j],
            device_id={"ep": flip(me, 1)},
        )

    def z_copy(source, target, part):
        rows = pl.ds(part * (tokens // 2), tokens // 2)
        return pltpu.make_async_remote_copy(
            zraw.at[source, rows],
            zraw.at[source, rows],
            z_send.at[source, part],
            z_recv.at[source, part],
            device_id={"ep": target},
        )

    def z_own(target, part, sem):
        rows = pl.ds(part * (tokens // 2), tokens // 2)
        return pltpu.make_async_remote_copy(
            x_ref.at[rows],
            zraw.at[me, rows],
            sem,
            z_recv.at[me, part],
            device_id={"ep": target},
        )

    def z_side(source, target):
        return pltpu.make_async_remote_copy(
            zraw.at[source],
            zraw.at[source],
            side_send.at[source],
            z_recv.at[source, 0],
            device_id={"ep": target},
        )

    parity = me % 2
    last = ep - 1
    spare = flip(me - parity, 2)
    other = spare + 1

    def wide_copy(j, target, start_full):
        return pltpu.make_async_remote_copy(
            full.at[0, j] if start_full else afull.at[j],
            afull.at[j],
            sent.at[4 if start_full else 5],
            a_recv.at[j],
            device_id={"ep": target},
        )

    def corner_copy(target, start_full):
        return pltpu.make_async_remote_copy(
            full.at[0, 3] if start_full else corner,
            corner,
            sent.at[14 if start_full else 15],
            b_recv.at[0],
            device_id={"ep": target},
        )

    def index_of(place):
        middle = jnp.where(place == 2, 3 - parity, place + 1)
        return jnp.where(place < 2, place, jnp.where(place == last, 2 + parity, middle))

    loads[0].wait()
    loads[1].wait()
    routes = routes_ref[...].astype(F32)
    named_ref[0:2, :] = routes
    named_ref[2:8, :] = jnp.full((6, tokens), -1.0, F32)
    full[0, 0] = x_ref[...]
    with scope("barrier"):
        pl.semaphore_wait(barrier, ep - 1 + tp - 1)

    for step in range(2):
        for j in direct:
            own_spread(j, (j - 1 + step) % 2).start()
    for i in range(1, ep):
        route_copy(i).start()

    for part in range(2):

        @pl.when(me < ep - 2)
        def _():
            z_own(me + 2, part, sent.at[16]).start()

        @pl.when(me >= 2)
        def _():
            z_own(me - 2, part, sent.at[17]).start()

    to_partner(0).start()
    rall[me] = named_ref[...]

    half = span // 2

    def piece(start, at, size):
        return pl.ds(pl.multiple_of(start + at * size, size), size)

    def spread(group, j, turn):
        rows = piece(group * span, (j - 1 + turn) % 2, half)
        return pltpu.make_async_remote_copy(
            tok.at[0, rows],
            tok.at[j, rows],
            sent.at[6],
            tok_rest.at[group - 2] if turn else tok_recv.at[group - 2, j - 1],
            device_id={"tp": flip(mine, j)},
        )

    def onward(group, j):
        part = piece(group * span, j - 1, half)
        return pltpu.make_async_remote_copy(
            tok.at[j, part],
            tok.at[3, part],
            sent.at[7],
            fwd_recv.at[group - 2],
            device_id={"tp": flip(mine, 3 - j)},
        )

    def share(group, j):
        return pltpu.make_async_remote_copy(
            hid.at[0, block(group, span)],
            hid.at[j, block(group, span)],
            sent.at[8],
            hid_recv.at[group, j - 1],
            device_id={"tp": flip(mine, j)},
        )

    def share_onward(group, j):
        part = piece(group * span, j - 1, half)
        return pltpu.make_async_remote_copy(
            hid.at[j, part],
            hid.at[3, part],
            sent.at[9],
            hidf_recv.at[group],
            device_id={"tp": flip(mine, 3 - j)},
        )

    def give_back(place, i):
        return pltpu.make_async_remote_copy(
            outb.at[block(place, span)],
            ret.at[block(i, span)],
            sent.at[10],
            ret_recv.at[0],
            device_id={"ep": flip_by(me, i, ep)},
        )

    tile = length // PARTS
    tile_half = tile // 2

    def head_spread(part, j, turn):
        rows = piece(part * tile, (j - 1 + turn) % 2, tile_half)
        return pltpu.make_async_remote_copy(
            hm.at[0, rows],
            hm.at[j, rows],
            sent.at[11],
            head_rest.at[part] if turn else head_recv.at[part, j - 1],
            device_id={"tp": flip(mine, j)},
        )

    def head_onward(part, j):
        rows = piece(part * tile, j - 1, tile_half)
        return pltpu.make_async_remote_copy(
            hm.at[j, rows],
            hm.at[3, rows],
            sent.at[12],
            hfwd_recv.at[part],
            device_id={"tp": flip(mine, 3 - j)},
        )

    def chain(h):
        return pltpu.make_async_remote_copy(
            st_out.at[h],
            st_in.at[h],
            sent.at[13],
            st_recv.at[h],
            device_id={"ep": me + 1},
        )

    many = pl.ds(0, len(direct))

    def pass_along(distance, part):
        below, above = me - 2 * distance, me + 2 * distance

        @pl.when(below >= 0)
        def _():
            with scope("F"):
                z_copy(below, me, part).wait_recv()

            @pl.when(me < ep - 2)
            def _():
                z_copy(below, me + 2, part).start()

            if part:
                z_side(below, flip(me, 1)).start()

        @pl.when(above < ep)
        def _():
            with scope("F"):
                z_copy(above, me, part).wait_recv()

            @pl.when(me >= 2)
            def _():
                z_copy(above, me - 2, part).start()

            if part:
                z_side(above, flip(me, 1)).start()

    def choose(source, rows):
        places = lax.broadcasted_iota(jnp.int32, (span, tokens), 0).astype(F32)
        hit = places == pos_ref[pl.ds(source, 1), :]
        return dot(hit.astype(F32).astype(BF16), rows).astype(BF16)

    def send_group(group):
        index = index_of(group)
        source = flip_by(me, index, ep)

        @pl.when(group == 2)
        def _():
            pass_along(1, 1)

        @pl.when((group > 2) & (index % 2 == 0))
        def _():
            pass_along(index // 2, 0)
            pass_along(index // 2, 1)

        @pl.when(index % 2 == 1)
        def _():
            with scope("S"):
                z_side(source, me).wait_recv()

        tok[0, block(group, span), :] = choose(source, zraw[source])
        for j in direct:
            spread(group, j, 0).start()

    def relay_own():
        for j in direct:
            with scope("O"):
                own_spread(j, (j - 1) % 2).wait_recv()
            if square:
                own_onward(j).start()
        pass_along(1, 0)
        for j in direct:
            with scope("O"):
                own_spread(j, j % 2).wait_recv()
            to_partner(j).start()

    def take_own():
        if square:
            with scope("O"):
                for j in direct:
                    own_onward(j).wait_recv()
            to_partner(3).start()
        for j in range(tp):
            tok[j, 0:span, :] = choose(me, full[0, j])

    def take_wide():
        @pl.when(parity == 1)
        def _():
            with scope("A"):
                z_side(spare, me).wait_recv()
                for j in range(1, tp):
                    wide_copy(j, me, False).wait_recv()

        rows = block(last, span)
        tok[0, rows, :] = choose(spare, zraw[spare])
        for j in range(1, tp):
            tok[j, rows, :] = choose(spare, afull[j])

    def take_partner():
        with scope("P"):
            for j in range(tp):
                to_partner(j).wait_recv()
        for j in range(tp):
            tok[j, span : 2 * span, :] = choose(flip(me, 1), full[1, j])

    def relay_group(group):
        if square:
            for j in direct:
                with scope("R"):
                    spread(group, j, 0).wait_recv()
                onward(group, j).start()

    def full_relay(group):
        rows = block(group, span)

        @pl.when(group > 2)
        def _():
            settled(tok.at[3, rows], fwd_recv.at[group - 2]).wait_recv()

        @pl.when(group == 2)
        def _():
            for j in direct:
                spread(group, j, 0).wait_recv()

            @pl.when(parity == 0)
            def _():
                corner_copy(me, False).wait_recv()

            tok[3, rows, :] = choose(other, corner[...])

    def collect_group(group):
        with scope("C"):
            if square:
                full_relay(group)
            else:
                for j in direct:
                    spread(group, j, 0).wait_recv()
            settled(tok.at[many, piece(0, 0, half)], tok_rest.at[group - 2]).wait_recv()

    def relay_share(group):
        if square:
            for j in direct:
                with scope("Q"):
                    share(group, j).wait_recv()
                share_onward(group, j).start()

    def expand(group):
        rows = block(group, span)
        gate = jnp.zeros((span, units), F32)
        up = jnp.zeros((span, units), F32)
        squares = jnp.zeros((span, 1), F32)
        for j in range(tp):
            piece = tok[j, rows, :]
            columns = pl.ds(pl.multiple_of(flip(mine, j) * width, width), width)
            gate += dot(piece, wg_ref[:, columns], ((1,), (1,)))
            up += dot(piece, wu_ref[:, columns], ((1,), (1,)))
            wide = piece.astype(F32)
            squares += jnp.sum(wide * wide, axis=1, keepdims=True)
        inverse = lax.rsqrt(squares / model_width + EPSILON)
        hid[0, rows, :] = (jax.nn.silu(gate * inverse) * (up * inverse)).astype(BF16)
        for j in direct:
            share(group, j).start()

    def contract(group):
        rows = block(group, span)
        with scope("K"):
            if square:
                settled(hid.at[3, block(group, span)], hidf_recv.at[group]).wait_recv()
            else:
                for j in direct:
                    share(group, j).wait_recv()
        total = jnp.zeros((span, width), F32)
        for j in range(tp):
            at = pl.ds(pl.multiple_of(flip(mine, j) * units, units), units)
            total += dot(hid[j, rows, :], wd_ref[at, :])
        outb[rows, :] = total.astype(BF16)

        @pl.when(group > 0)
        def _():
            give_back(group, index_of(group)).start()

    for at in range(2, 6):
        loads[at].wait()
    forget = forget_ref[...]
    decay_log = jnp.minimum(forget, 0.0) - jnp.log1p(jnp.exp(-jnp.abs(forget)))
    head_part = decay_log.astype(BF16)
    rest = decay_log - head_part.astype(F32)
    mid_part = rest.astype(BF16)
    low_part = (rest - mid_part.astype(F32)).astype(BF16)
    upper = lax.broadcasted_iota(jnp.int32, (length, length), 0) <= lax.broadcasted_iota(
        jnp.int32, (length, length), 1
    )
    upper = upper.astype(F32).astype(BF16)
    cumulative = dot(head_part, upper) + dot(mid_part, upper) + dot(low_part, upper)
    cum_ref[...] = cumulative
    a_ref[...] = in_ref[...] - cumulative

    strict = lax.broadcasted_iota(jnp.int32, (tokens, tokens), 0) < lax.broadcasted_iota(
        jnp.int32, (tokens, tokens), 1
    )
    strict = strict.astype(F32).astype(BF16)
    order = lax.broadcasted_iota(jnp.int32, (ep, tokens), 0)
    experts = (order ^ me).astype(F32)
    one = jnp.ones((ep, tokens), F32)
    none = jnp.zeros((ep, tokens), F32)
    first = jnp.where(experts == routes[0:1, :], one, none)
    second = jnp.where(experts == routes[1:2, :], one, none)
    places = (order * span).astype(F32) + dot((first + second).astype(BF16), strict)
    slot_row_ref[0:1, :] = jnp.sum(first * places, axis=0, keepdims=True)
    slot_row_ref[1:2, :] = jnp.sum(second * places, axis=0, keepdims=True)

    loads[6].wait()
    loads[7].wait()

    def summarise(h, carry):
        keys = k_ref[:, block(h, qk)]
        values = v_ref[:, block(h, vw)]
        log_in = a_ref[pl.ds(h, 1), :]
        top = jnp.max(log_in, axis=1, keepdims=True)
        weighted = keys.astype(F32) * jnp.exp(upright(log_in) - top)
        local[h, 0:qk, :] = dot(weighted.astype(BF16), values, ((0,), (0,)))
        normal = jnp.sum(weighted, axis=0, keepdims=True)
        local[h, qk : qk + 8, 0:qk] = jnp.broadcast_to(normal, (8, qk))
        decay = cum_ref[pl.ds(h, 1), :][:, length - 1 : length]
        local[h, qk + 8 : qk + 16, :] = jnp.broadcast_to(top + decay, (8, vw))
        return carry

    with scope("summarise"):
        lax.fori_loop(0, head_count, summarise, 0)

    @pl.when(me == 0)
    def _():
        st_in[:, 0 : qk + 8, :] = jnp.zeros((head_count, qk + 8, vw), F32)
        st_in[:, qk + 8 : qk + 16, :] = jnp.full((head_count, 8, vw), LOG_FLOOR, F32)

    def carry_on(h, carry):
        @pl.when(me > 0)
        def _():
            with scope("chainwait"):
                chain(h).wait_recv()

        decay = cum_ref[pl.ds(h, 1), :][:, length - 1 : length]
        carried_max = st_in[h, qk + 8 : qk + 9, :] + decay
        own_max = local[h, qk + 8 : qk + 9, :]
        new_max = jnp.maximum(carried_max, own_max)
        keep = jnp.exp(carried_max - new_max)
        add = jnp.exp(own_max - new_max)
        st_out[h, 0:qk, :] = keep * st_in[h, 0:qk, :] + add * local[h, 0:qk, :]
        st_out[h, qk : qk + 8, 0:qk] = (
            keep[:, 0:qk] * st_in[h, qk : qk + 8, 0:qk]
            + add[:, 0:qk] * local[h, qk : qk + 8, 0:qk]
        )
        st_out[h, qk : qk + 8, qk:vw] = jnp.zeros((8, vw - qk), F32)
        st_out[h, qk + 8 : qk + 16, :] = jnp.broadcast_to(new_max, (8, vw))

        @pl.when(me < ep - 1)
        def _():
            chain(h).start()

        return carry

    def heads(h, carry):
        columns = block(h, vw)
        queries = q_ref[:, block(h, qk)]
        keys = k_ref[:, block(h, qk)]
        scale = qk**-0.5
        causal = lax.broadcasted_iota(jnp.int32, (length, length), 1) <= lax.broadcasted_iota(
            jnp.int32, (length, length), 0
        )
        log_in = jnp.where(causal, a_ref[pl.ds(h, 1), :], -jnp.inf)
        prior_max = st_in[h, qk + 8 : qk + 9, 0:1]
        top = jnp.maximum(prior_max, jnp.max(log_in, axis=1, keepdims=True))
        scores = dot(queries, keys, ((1,), (1,))) * scale * jnp.exp(log_in - top)
        carried = jnp.exp(prior_max - top) * scale
        memory = st_in[h, 0:qk, :]
        high = memory.astype(BF16)
        low = (memory - high.astype(F32)).astype(BF16)
        numerator = carried * (dot(queries, high) + dot(queries, low)) + dot(
            scores.astype(BF16), v_ref[:, columns]
        )
        normal = st_in[h, qk : qk + 1, 0:qk]
        denominator = carried * jnp.sum(
            queries.astype(F32) * normal, axis=1, keepdims=True
        ) + jnp.sum(scores, axis=1, keepdims=True)
        floor = jnp.exp(-(upright(cum_ref[pl.ds(h, 1), :]) + top))
        value = numerator / jnp.maximum(jnp.abs(denominator), floor)
        value = value * lax.rsqrt(jnp.mean(value * value, axis=1, keepdims=True) + EPSILON)
        gate = jax.nn.sigmoid(og_ref[:, columns].astype(F32))
        hm[0, :, columns] = (value * gain_ref[:, columns] * gate).astype(BF16)
        return carry

    for at in range(8, 14):
        loads[at].wait()

    with scope("routes"):
        settled(rall.at[pl.ds(0, ep - 1)], route_recv.at[0]).wait_recv()
    wanted = jnp.zeros((ep, tokens), F32) + me.astype(F32)
    named = (rall[:, 0, :] == wanted) | (rall[:, 1, :] == wanted)
    ahead = dot(jnp.where(named, one, none).astype(BF16), strict)
    pos_ref[...] = jnp.where(named, ahead, -one)

    def when_between(step, low, high):
        return pl.when((step >= low) & (step <= high))

    quarter = me // (ep // 4)
    slot = quarter * (7 - quarter) // 2 * (ep // 8)
    first_part = last
    early = (1,) if square else direct
    late = (1 - (me // 2) % 2) * jnp.minimum(me // 2, 1)
    final = last + 1 + ((me // 2) % 2) * jnp.minimum(me // 4, 1)
    tardy = late * (1 - parity)

    def turn(n):
        return jnp.where(n < 2, n, jnp.where(n == last, n, jnp.where(n == last - 1, 2, n + 1)))

    def turns(k):
        low = jnp.where(k == 2, 0, jnp.where(k == final, last, k - 2))
        high = jnp.where(k == last, k, k - 1)
        return low, jnp.where(k == 2, 2, jnp.where(k == final, last + 1, high))

    def busy(k):
        return (k == 2) | ((k >= 4) & (k <= last)) | (k == final)

    def absorb(n, carry):
        group = turn(n)

        @pl.when(group == 0)
        def _():
            take_own()

        @pl.when(group == 1)
        def _():
            take_partner()

        @when_between(group, 2, last - 1)
        def _():
            collect_group(group)

        @pl.when(group == last)
        def _():
            take_wide()

        with scope("expand"):
            expand(group)
        return carry

    def pass_share(n, carry):
        relay_share(turn(n))
        return carry

    def finish_group(n, carry):
        contract(turn(n))
        return carry

    def relay_heads(part):
        if square:
            for j in direct:
                with scope("HR"):
                    head_spread(part, j, 0).wait_recv()
                head_onward(part, j).start()

    def settle():
        settled(rall.at[pl.ds(0, ep - 1)], sent.at[0]).wait_send()
        settled(full.at[0, pl.ds(1, len(direct))], sent.at[1]).wait_send()
        settled(full.at[1], sent.at[3]).wait_send()

        @pl.when(parity == 0)
        def _():
            settled(afull.at[pl.ds(1, tp - 1)], sent.at[4]).wait_send()
            settled(afull.at[pl.ds(1, tp - 1)], sent.at[5]).wait_send()

        @pl.when(me < ep - 2)
        def _():
            settled(x_ref, sent.at[16]).wait_send()

        @pl.when(me >= 2)
        def _():
            settled(x_ref, sent.at[17]).wait_send()

        for distance in range(1, ep // 2):
            below, above = me - 2 * distance, me + 2 * distance

            @pl.when(below >= 0)
            def _():
                z_side(below, flip(me, 1)).wait_send()

                @pl.when(me < ep - 2)
                def _():
                    for part in range(2):
                        z_copy(below, me + 2, part).wait_send()

            @pl.when(above < ep)
            def _():
                z_side(above, flip(me, 1)).wait_send()

                @pl.when(me >= 2)
                def _():
                    for part in range(2):
                        z_copy(above, me - 2, part).wait_send()

        spread_rows = pl.ds(0, (ep - 3) * span)
        settled(tok.at[many, spread_rows], sent.at[6]).wait_send()
        settled(hid.at[many], sent.at[8]).wait_send()
        if square:
            settled(full.at[0, 3], sent.at[2]).wait_send()
            settled(tok.at[0, pl.ds(0, (ep - 4) * span)], sent.at[7]).wait_send()

            @pl.when(parity == 1)
            def _():
                settled(corner, sent.at[14]).wait_send()
                settled(corner, sent.at[15]).wait_send()

            settled(hid.at[0], sent.at[9]).wait_send()

        @pl.when(me < ep - 1)
        def _():
            settled(st_out, sent.at[13]).wait_send()

    def combine():
        returns = pl.ds(0, (ep - 1) * span)
        with scope("retwait"):
            settled(ret.at[returns], ret_recv.at[0]).wait_recv()
        ret[0:span, :] = outb[0:span, :]
        places = lax.broadcasted_iota(jnp.int32, (ret.shape[0], tokens), 0).astype(F32)
        total = jnp.zeros((tokens, width), F32)
        for route in range(weight_ref.shape[0]):
            hit = places == slot_row_ref[route : route + 1, :]
            picked = dot(hit.astype(F32).astype(BF16), ret[...], ((0,), (0,)))
            total += picked * upright(weight_ref[route : route + 1, :])
        exp_ref[...] = total.astype(BF16)
        settled(ret.at[returns], sent.at[10]).wait_send()

    def mix(part):
        rows = block(part, tile)
        with scope("M"):
            if not square:
                for j in direct:
                    head_spread(part, j, 0).wait_recv()
            settled(hm.at[many, piece(0, 0, tile_half)], head_rest.at[part]).wait_recv()

        def share_of(j):
            inputs = pl.ds(pl.multiple_of(flip(mine, j) * width, width), width)
            return dot(hm[j, rows, :], wm_ref[inputs, :])

        total = jnp.zeros((tile, width), F32)
        for j in range(tp - 1):
            total += share_of(j)
        partial[...] = total
        if square:
            with scope("M2"):
                settled(hm.at[3, rows], hfwd_recv.at[part]).wait_recv()
        mix_ref[rows, :] = (partial[...] + share_of(tp - 1)).astype(BF16)

    def step(k, carry):
        @pl.when(k == slot)
        def _():
            with scope("chain"):
                lax.fori_loop(0, head_count, carry_on, 0)
            with scope("heads"):
                lax.fori_loop(0, head_count // 2, heads, 0)

        @pl.when(k == jnp.minimum(slot + 1, last - 1))
        def _():
            with scope("heads"):
                lax.fori_loop(head_count // 2, head_count, heads, 0)

        @pl.when(k == 0)
        def _():
            relay_own()

        @pl.when(busy(k) & (k != last + 2))
        def _():
            lax.fori_loop(*turns(k), absorb, 0)

        @when_between(k, 3 if square else 2, last - 1)
        def _():
            relay_group(k)

        @when_between(k, first_part, first_part + PARTS - 1)
        def _():
            relay_heads(k - first_part)

        @pl.when((k == final) & (k == last + 2))
        def _():
            relay_share(last)

        @pl.when(busy(k - 1) & (k != last + 3))
        def _():
            lax.fori_loop(*turns(k - 1), finish_group, 0)

        if square:

            @pl.when((k == final - 1) & (parity == 0))
            def _():
                for j in (2, 3):
                    with scope("A3"):
                        wide_copy(j, me, False).wait_recv()
                    wide_copy(j, flip(me, 1), False).start()

        @when_between(k, 1, last - 2)
        def _():
            send_group(k + 1)

        @when_between(k, first_part - 1, first_part + PARTS - 2)
        def _():
            for j in direct:
                head_spread(k + 1 - first_part, j, 0).start()

        @pl.when(busy(k) & (k != last + 2))
        def _():
            lax.fori_loop(*turns(k), pass_share, 0)

        @when_between(k, 1, last - 2)
        def _():
            for j in direct:
                spread(k + 1, j, 1).start()

        @when_between(k, first_part - 1, first_part + PARTS - 2)
        def _():
            for j in direct:
                head_spread(k + 1 - first_part, j, 1).start()

        @pl.when((k == 2) & (parity == 0))
        def _():
            for j in early:
                wide_copy(j, flip(me, 2), True).start()

        if square:

            @pl.when((k == 2 + 3 * late) & (parity == 0))
            def _():
                for j in (2, 3):
                    wide_copy(j, flip(me, 2), True).start()

            @pl.when((k == 2) & (parity == 1))
            def _():
                corner_copy(flip(me, 2), True).start()

            @pl.when((k == last - 1) & (parity == 1))
            def _():
                with scope("B"):
                    corner_copy(me, False).wait_recv()
                corner_copy(flip(me, 1), False).start()

        @pl.when((k == last - 1) & (parity == 0))
        def _():
            for j in early:
                with scope("A"):
                    wide_copy(j, me, False).wait_recv()
                wide_copy(j, flip(me, 1), False).start()

        @pl.when((k == final - 1) & (k == last + 1))
        def _():
            absorb(last, 0)

        @pl.when((k == final) & (k == last + 2))
        def _():
            contract(last)

        @pl.when(k == first_part + PARTS)
        def _():
            settle()

        @pl.when((k == first_part + PARTS) & (tardy == 0))
        def _():
            combine()

        @pl.when(k > first_part)
        def _():
            mix(k - first_part - 1)

        @pl.when((k == first_part + PARTS) & (tardy == 1))
        def _():
            combine()

        return carry

    lax.fori_loop(0, first_part + PARTS + 1, step, 0)

    with scope("fin"):
        settled(hm.at[many], sent.at[11]).wait_send()
        if square:
            settled(hm.at[0], sent.at[12]).wait_send()


def body(
    query_rows,
    key_rows,
    value_rows,
    in_gate,
    forget_gate,
    out_gate,
    head_gain,
    mix_weight,
    expert_input,
    routes,
    route_weight,
    gate_weight,
    up_weight,
    down_weight,
):
    ep, tp = lax.axis_size("ep"), lax.axis_size("tp")
    head_count, length = in_gate.shape
    token_count, fanout = routes.shape
    width = expert_input.shape[1]
    units = gate_weight.shape[1]
    capacity = 2 * token_count * fanout // ep
    slot_count = ep * capacity
    qk = query_rows.shape[1] // head_count
    vw = value_rows.shape[1] // head_count

    vmem = pl.BlockSpec(memory_space=pltpu.VMEM)
    anywhere = pl.BlockSpec(memory_space=pl.ANY)
    dma = pltpu.SemaphoreType.DMA
    gate_local, up_local, down_local = gate_weight[0], up_weight[0], down_weight[0]
    small = (expert_input, routes.T, route_weight.T, in_gate, forget_gate, head_gain[None, :])
    big = (query_rows, key_rows, value_rows, out_gate, gate_local, up_local, down_local, mix_weight)
    state = (head_count, qk + PAD, vw)
    direct = 2 if tp == 4 else tp - 1
    return pl.pallas_call(
        functools.partial(kernel, ep, tp, head_count, mix_weight.shape[0]),
        out_shape=(
            pltpu.VMEM((length, width), BF16),
            pltpu.VMEM((token_count, width), BF16),
        ),
        in_specs=[anywhere] * 14,
        out_specs=(vmem, vmem),
        scratch_shapes=[pltpu.VMEM(array.shape, array.dtype) for array in small + big]
        + [
            pltpu.VMEM((head_count, length), F32),
            pltpu.VMEM((head_count, length), F32),
            pltpu.VMEM((fanout, token_count), F32),
            pltpu.VMEM((ep, token_count), F32),
            pltpu.VMEM((8, token_count), F32),
            pltpu.VMEM((ep, 8, token_count), F32),
            pltpu.VMEM((2, tp, token_count, width), BF16),
            pltpu.VMEM((ep, token_count, width), BF16),
            pltpu.VMEM((tp, token_count, width), BF16),
            pltpu.VMEM((token_count, width), BF16),
            pltpu.VMEM((tp, slot_count, width), BF16),
            pltpu.VMEM((tp, slot_count, units), BF16),
            pltpu.VMEM((slot_count, width), BF16),
            pltpu.VMEM((slot_count, width), BF16),
            pltpu.VMEM((tp, length, width), BF16),
            pltpu.VMEM(state, F32),
            pltpu.VMEM(state, F32),
            pltpu.VMEM(state, F32),
            pltpu.VMEM((length // PARTS, width), F32),
            dma((14,)),
            dma((18,)),
            dma((1,)),
            dma((direct, 2)),
            dma((2,)),
            dma((tp,)),
            dma((ep, 2)),
            dma((ep,)),
            dma((ep, 2)),
            dma((tp,)),
            dma((1,)),
            dma((ep - 3, direct)),
            dma((ep - 3,)),
            dma((ep - 3,)),
            dma((ep, direct)),
            dma((ep,)),
            dma((1,)),
            dma((PARTS, direct)),
            dma((PARTS,)),
            dma((PARTS,)),
            dma((head_count,)),
        ],
        compiler_params=pltpu.CompilerParams(
            collective_id=0, has_side_effects=True, vmem_limit_bytes=58000 * 1024
        ),
    )(
        *small,
        *big,
    )


def solution(mesh):
    in_specs = (
        P("ep", "tp"),
        P("ep", "tp"),
        P("ep", "tp"),
        P("tp", "ep"),
        P("tp", "ep"),
        P("ep", "tp"),
        P("tp"),
        P(None, "tp"),
        P("ep", "tp"),
        P("ep", None),
        P("ep", None),
        P("ep", "tp", None),
        P("ep", "tp", None),
        P("ep", None, "tp"),
    )
    out_specs = (P("ep", "tp"), P("ep", "tp"))
    return jax.shard_map(body, mesh=mesh, in_specs=in_specs, out_specs=out_specs, check_vma=False)
```
